512 devices in a mesh: ep: 128 (over z, y, core), tp: 4 (over x).
Axes of the slice: x: 4, y: 8, z: 8, core: 2. Of those that a mesh axis runs over, the one named last changes fastest.
Arguments:
- tokens: bfloat16 [2048, 1024], P('ep', 'tp'), may hold values from -75 to 75
- gain_mix: float32 [1024], replicated, may hold values from 0.1 to 1.9
- w_query: bfloat16 [1024, 512], P(None, 'tp'), may hold values from -0.1875 to 0.1875
- w_key: bfloat16 [1024, 512], P(None, 'tp'), may hold values from -0.1875 to 0.1875
- w_value: bfloat16 [1024, 512], P(None, 'tp'), may hold values from -0.1875 to 0.1875
- w_outgate: bfloat16 [1024, 512], P(None, 'tp'), may hold values from -0.1875 to 0.1875
- w_input_gate: bfloat16 [1024, 4], P(None, 'tp'), may hold values from -0.1875 to 0.1875
- w_forget_gate: bfloat16 [1024, 4], P(None, 'tp'), may hold values from -0.1875 to 0.1875
- w_mix_out: bfloat16 [512, 1024], P(None, 'tp'), may hold values from -0.25 to 0.25
- cell_state: float32 [2048, 4, 128, 128], P('ep', 'tp'), may hold values from -3 to 3
- norm_state: float32 [2048, 4, 128], P('ep', 'tp'), may hold values from -3 to 3
- max_state: float32 [2048, 4], P('ep', 'tp'), may hold values from -2 to 143
- gain_ffn: float32 [1024], replicated, may hold values from 0.1 to 1.9
- route_ids: int32 [2048, 2], P('ep'), may hold values from 0 to 127, all different within a row; in each aligned block of 16 rows (0 to 15, 16 to 31, ...) no two rows name the same one
- route_logits: float32 [2048, 2], P('ep'), may hold values from -5 to 5
- expert_gate: bfloat16 [128, 1024, 1408], P('ep', None, 'tp'), may hold values from -0.1875 to 0.1875
- expert_up: bfloat16 [128, 1024, 1408], P('ep', None, 'tp'), may hold values from -0.1875 to 0.1875
- expert_down: bfloat16 [128, 1408, 1024], P('ep', 'tp'), may hold values from -0.15625 to 0.15625
- dense_gate: bfloat16 [1024, 3072], P('tp', 'ep'), may hold values from -0.1875 to 0.1875
- dense_up: bfloat16 [1024, 3072], P('tp', 'ep'), may hold values from -0.1875 to 0.1875
- dense_down: bfloat16 [3072, 1024], P('ep', 'tp'), may hold values from -0.3125 to 0.3125
- dense_mix: bfloat16 [1024], P('tp'), may hold values from -0.1875 to 0.1875
Outputs:
- layer_out: bfloat16 [2048, 1024], P('ep', 'tp')
The draws below stay inside these ranges and needn't reach their ends.
Inputs may be any that keep to these rules, and one draw needn't show every extreme that they name: `route_ids`: each row names 2 different experts. Among the 16 tokens of one index of ep no expert is named more than 1 times, and in every draw some expert is named exactly 1 times by the tokens of one index of ep.
All inputs are finite; a program needn't handle non-finite values.
Results may differ from the reference program's by a relative error of at most 0.013.
Values may be sent and summed in bfloat16 or wider, within the bound.
No kernel may reach another device: no remote copies, remote signals or barrier semaphores. Data moves between devices by JAX's collectives and lax.ppermute only.
A program may use at most 64 MiB of HBM per device.

```python
import math
import jax
import jax.numpy as jnp
import numpy as np
from jax import lax

D = 1024
HEADS = 4
HEAD = 128
FF_EXP = 1408
DENSE_FF = 3072
SEQ_DEV = 16
TOP = 2
CAP = 1
WIDTH = 512
BATCH = 2048
EXPERTS = 128
N_TP = 4


def draw_tokens(key, part):
    key_base, key_group, key_block = jax.random.split(key, 3)
    base = jnp.clip(jax.random.normal(key_base, (BATCH, D), jnp.float32), -5.0, 5.0)
    group_scale = jnp.exp(jax.random.uniform(key_group, (D // 16,), jnp.float32, -1.1, 1.1))
    block_scale = jnp.exp(jax.random.uniform(key_block, (4,), jnp.float32, -1.1, 1.1))
    columns = jnp.arange(D)
    values = base * group_scale[columns // 16][None, :] * block_scale[columns // (D // 4)][None, :]
    return values.astype(jnp.bfloat16)


def draw_max_state(key, part):
    key_base = jax.random.fold_in(key, 0)
    base = jax.random.uniform(key_base, (BATCH, HEADS), jnp.float32, -2.0, 3.0)
    return base


def shard_levels(stream_key, dims, cuts, low, top_value):
    level, own = 1.0, jax.random.fold_in(stream_key, 6)
    for position, parts in cuts:
        heights = jnp.exp(jax.random.uniform(jax.random.fold_in(own, position), (parts,), jnp.float32, low / len(cuts), top_value / len(cuts)))
        level = level * jnp.repeat(heights, dims[position] // parts).reshape([-1 if axis == position else 1 for axis in range(len(dims))])
    return level


def deal_out(stream_key, own, number, rows, amount, top, limit, skew):
    sequence = jax.random.permutation(stream_key, amount)
    heavy_load, ordinary = load_shares(amount, rows * top, limit, skew, True), load_shares(amount, rows * top, limit, skew, False)
    places = jnp.arange(amount)

    def named(tallies, rotation):
        used = int((tallies > 0).sum())
        fixed = max(1, used // 4)
        passed = fixed + (places - fixed + rotation * (used - fixed)) % max(1, amount - fixed)
        return jnp.zeros((amount,), jnp.int32).at[sequence[jnp.where(places < fixed, places, passed)]].set(jnp.asarray(tallies, jnp.int32))

    tallies = jnp.where(number % 4 == 0, named(heavy_load, number // 4), named(ordinary, number - number // 4 - 1))
    mixed = jax.random.permutation(jax.random.fold_in(own, 3), amount)
    giver, sink = mixed[0:amount // 2 * 2:2], mixed[1:amount // 2 * 2:2]
    room = jnp.minimum(tallies[giver] - 1, limit - tallies[sink]) // 2
    room = jnp.where((giver == sequence[0]) | (sink == sequence[0]) | (tallies[sink] == 0), 0, jnp.maximum(room, 0))
    passed = jax.random.randint(jax.random.fold_in(own, 4), (amount // 2,), 0, 1 << 20) % (room + 1)
    tallies = tallies.at[giver].add(-passed).at[sink].add(passed)
    members = jnp.searchsorted(jnp.cumsum(tallies), jnp.arange(rows * top), side="right").astype(jnp.int32)
    table = members.reshape(top, rows).T
    table = table[jax.random.permutation(jax.random.fold_in(own, 1), rows)]
    rotation = jax.random.randint(jax.random.fold_in(own, 2), (rows, 1), 0, top)
    return jnp.take_along_axis(table, (jnp.arange(top)[None, :] + rotation) % top, axis=1)


def load_shares(count, total, most, skew, full):
    weights = [(1 << 20) // math.isqrt(standing ** skew) + 1 for standing in range(1, count + 1)]
    largest = most if full else min(most, max(-(-total // count), total * weights[0] // sum(weights)))
    least = 1 if total - largest >= count - 1 else 0
    counts, spare = [largest] + [least] * (count - 1), total - largest - least * (count - 1)
    while spare > 0:
        free = [i for i in range(1, count) if counts[i] < largest] or [i for i in range(1, count) if counts[i] < most]
        mass, budget = sum([weights[i] for i in free]), spare
        for i in free:
            more = min(most - counts[i], max(1, budget * weights[i] // mass), spare)
            counts[i] = counts[i] + more
            spare = spare - more
    return np.array(counts)


def normal_values(key, dims, scale, bound, shards=(), held_as=jnp.bfloat16):
    factor_of = shard_levels(key, dims, shards, -0.22, 0.18) if shards else 1.0
    drawn = jax.random.normal(key, dims, jnp.float32) * scale * factor_of
    return jnp.minimum(jnp.maximum(drawn, -bound), bound).astype(held_as)


def setup_inputs(seed: int = 0) -> dict:
    key_of = jax.random.split(jax.random.key(seed), 23)
    tokens = draw_tokens(jax.random.fold_in(key_of[22], 71), 0)
    gain_mix = jnp.clip(1.0 + 0.18 * jax.random.normal(key_of[1], (D,), jnp.float32), 0.1, 1.9)
    w_query = normal_values(key_of[2], (D, WIDTH), D ** -0.5, 0.1875, ((1, 4),))
    w_key = normal_values(key_of[3], (D, WIDTH), D ** -0.5, 0.1875, ((1, 4),))
    w_value = normal_values(key_of[4], (D, WIDTH), D ** -0.5, 0.1875, ((1, 4),))
    w_outgate = normal_values(key_of[5], (D, WIDTH), D ** -0.5, 0.1875, ((1, 4),))
    w_input_gate = normal_values(key_of[6], (D, HEADS), D ** -0.5, 0.1875, ((1, 4),))
    w_forget_gate = normal_values(key_of[7], (D, HEADS), D ** -0.5, 0.1875, ((1, 4),))
    w_mix_out = normal_values(key_of[8], (WIDTH, D), WIDTH ** -0.5, 0.25, ((1, 4),))
    cell_state = normal_values(key_of[9], (BATCH, HEADS, HEAD, HEAD), 0.5, 3.0, ((0, 128), (1, 4)), jnp.float32)
    norm_state = normal_values(key_of[10], (BATCH, HEADS, HEAD), 0.5, 3.0, ((0, 128), (1, 4)), jnp.float32)
    max_state = draw_max_state(jax.random.fold_in(key_of[22], 71), 0)
    gain_ffn = jnp.clip(1.0 + 0.18 * jax.random.normal(key_of[12], (D,), jnp.float32), 0.1, 1.9)
    route_ids_keys = jax.random.split(jax.random.fold_in(key_of[13], 1), BATCH // SEQ_DEV)
    route_ids_turns = jax.random.permutation(jax.random.fold_in(key_of[13], 3), BATCH // SEQ_DEV)
    route_ids = jax.vmap(lambda own, number: deal_out(jax.random.fold_in(key_of[13], 2), own, number, SEQ_DEV, EXPERTS, TOP, CAP, 2))(route_ids_keys, route_ids_turns).reshape((BATCH, TOP))
    route_logits = normal_values(key_of[14], (BATCH, TOP), 1.0, 5.0, ((0, 128),), jnp.float32)
    expert_gate = normal_values(key_of[15], (EXPERTS, D, FF_EXP), D ** -0.5, 0.1875, ((0, 128), (2, 4)))
    expert_up = normal_values(key_of[16], (EXPERTS, D, FF_EXP), D ** -0.5, 0.1875, ((0, 128), (2, 4)))
    expert_down = normal_values(key_of[17], (EXPERTS, FF_EXP, D), FF_EXP ** -0.5, 0.15625, ((0, 128), (1, 4)))
    dense_gate = normal_values(key_of[18], (D, DENSE_FF), D ** -0.5, 0.1875, ((0, 4), (1, 128)))
    dense_up = normal_values(key_of[19], (D, DENSE_FF), D ** -0.5, 0.1875, ((0, 4), (1, 128)))
    dense_down = normal_values(key_of[20], (DENSE_FF, D), (DENSE_FF // 8) ** -0.5, 0.3125, ((0, 128), (1, 4)))
    dense_mix = normal_values(key_of[21], (D,), D ** -0.5, 0.1875, ((0, 4),))
    return dict(tokens=tokens, gain_mix=gain_mix, w_query=w_query, w_key=w_key, w_value=w_value, w_outgate=w_outgate, w_input_gate=w_input_gate, w_forget_gate=w_forget_gate, w_mix_out=w_mix_out, cell_state=cell_state, norm_state=norm_state, max_state=max_state, gain_ffn=gain_ffn, route_ids=route_ids, route_logits=route_logits, expert_gate=expert_gate, expert_up=expert_up, expert_down=expert_down, dense_gate=dense_gate, dense_up=dense_up, dense_down=dense_down, dense_mix=dense_mix)


epsilon = 1e-06
highest = lax.Precision.HIGHEST

def rms_norm(rows, gain):
    values = rows.astype(jnp.float32)
    scale = lax.rsqrt(lax.optimization_barrier(jnp.mean(values * values, axis=-1, keepdims=True)) + epsilon)
    return (values * scale * gain).astype(jnp.bfloat16)

def reference(tokens, gain_mix, w_query, w_key, w_value, w_outgate, w_input_gate, w_forget_gate, w_mix_out, cell_state, norm_state, max_state, gain_ffn, route_ids, route_logits, expert_gate, expert_up, expert_down, dense_gate, dense_up, dense_down, dense_mix):
    normed_mix = rms_norm(tokens, gain_mix)

    def project(weight):
        return jnp.dot(normed_mix, weight, preferred_element_type=jnp.float32)
    query_rows = project(w_query).reshape(BATCH, HEADS, HEAD)
    key_rows = project(w_key).reshape(BATCH, HEADS, HEAD) * HEAD ** (-0.5)
    value_rows = project(w_value).reshape(BATCH, HEADS, HEAD)
    out_gate = project(w_outgate)
    input_gate = project(w_input_gate)
    carried = jax.nn.log_sigmoid(project(w_forget_gate)) + max_state
    stabilizer = jnp.maximum(carried, input_gate)
    weight_old = jnp.exp(carried - stabilizer)
    weight_new = jnp.exp(input_gate - stabilizer) * lax.optimization_barrier(jnp.sum(query_rows * key_rows, axis=-1))
    cell_read = jnp.einsum('bhd,bhde->bhe', query_rows, cell_state, precision=highest)
    numerator = weight_old[..., None] * cell_read + weight_new[..., None] * value_rows
    denominator = weight_old * lax.optimization_barrier(jnp.sum(query_rows * norm_state, axis=-1)) + weight_new
    cell_out = numerator / jnp.maximum(jnp.abs(denominator), 1.0)[..., None]
    mixed = (jax.nn.sigmoid(out_gate) * cell_out.reshape(BATCH, WIDTH)).astype(jnp.bfloat16)
    resid = (tokens.astype(jnp.float32) + jnp.dot(mixed, w_mix_out, preferred_element_type=jnp.float32)).astype(jnp.bfloat16)
    normed_ffn = rms_norm(resid, gain_ffn)
    route_weight = jax.nn.sigmoid(route_logits - route_logits[:, ::-1])
    token_rows = jnp.repeat(normed_ffn, TOP, axis=0)
    flat_ids = route_ids.reshape(-1).astype(jnp.int32)

    def apply_expert(assignment):
        token_row, expert_id = assignment
        gate_rows = jnp.dot(token_row, expert_gate[expert_id], preferred_element_type=jnp.float32)
        up_rows = jnp.dot(token_row, expert_up[expert_id], preferred_element_type=jnp.float32)
        hidden = (jax.nn.silu(gate_rows) * up_rows).astype(jnp.bfloat16).reshape(N_TP, FF_EXP // N_TP)
        down_rows = expert_down[expert_id].reshape(N_TP, FF_EXP // N_TP, D).astype(jnp.float32)
        blocks = jnp.einsum('jf,jfd->jd', hidden.astype(jnp.float32), down_rows, precision=highest)
        blocks = lax.optimization_barrier(blocks.astype(jnp.bfloat16))
        return lax.optimization_barrier(jnp.sum(blocks.astype(jnp.float32), axis=0)).astype(jnp.bfloat16)
    expert_result = lax.map(apply_expert, (token_rows, flat_ids)).reshape(BATCH, TOP, D)
    moe = lax.optimization_barrier(jnp.sum(route_weight[..., None] * expert_result.astype(jnp.float32), axis=1))
    dense_g = jnp.dot(normed_ffn, dense_gate, preferred_element_type=jnp.float32)
    dense_u = jnp.dot(normed_ffn, dense_up, preferred_element_type=jnp.float32)
    dense_hidden = (jax.nn.silu(dense_g) * dense_u).astype(jnp.bfloat16)
    dense_out = jnp.dot(dense_hidden, dense_down, preferred_element_type=jnp.float32)
    mix_gate = jax.nn.sigmoid(jnp.dot(normed_ffn, dense_mix, preferred_element_type=jnp.float32))
    total = resid.astype(jnp.float32) + moe + mix_gate[:, None] * dense_out
    return total.astype(jnp.bfloat16)
```

```python
import jax
import jax.numpy as jnp
from jax import lax
from jax.sharding import Mesh, PartitionSpec as P

HEAD = 128
TOP = 2

epsilon = 1e-06
highest = lax.Precision.HIGHEST
f32 = jnp.float32
bf16 = jnp.bfloat16

FAR = ("zh", "yh")
NEAR = ("zl", "yl", "c")
EP = ("zh", "zl", "yh", "yl", "c")


def exchange(blocks, axis):
    return lax.all_to_all(blocks, axis, 0, 0, tiled=True)


def to_all(shard, size):
    return jnp.broadcast_to(shard[None], (size, *shard.shape))


def side_by_side(blocks):
    count, rows, columns = blocks.shape
    return jnp.moveaxis(blocks, 0, 1).reshape(rows, count * columns)


def rms_norm(rows, gain):
    values = rows.astype(f32)
    scale = lax.rsqrt(jnp.mean(values * values, axis=-1, keepdims=True) + epsilon)
    return (values * scale * gain).astype(bf16)


def dot(a, b):
    return jnp.dot(a, b, preferred_element_type=f32)


def local(
    tokens,
    gain_mix,
    w_query,
    w_key,
    w_value,
    w_outgate,
    w_input_gate,
    w_forget_gate,
    w_mix_out,
    cell_state,
    norm_state,
    max_state,
    gain_ffn,
    route_ids,
    route_logits,
    expert_gate,
    expert_up,
    expert_down,
    dense_gate,
    dense_up,
    dense_down,
    dense_mix,
):
    seqs, quarter = tokens.shape
    tp = lax.axis_size("x")
    far = lax.axis_size(FAR)
    near = lax.axis_size(NEAR)
    experts = lax.axis_size(EP)
    me = lax.axis_index("x")
    columns = dense_gate.shape[1]
    slim = columns // tp

    full_tokens = side_by_side(exchange(to_all(tokens, tp), "x"))

    extra = jnp.concatenate([dense_mix[None], jnp.zeros((7, quarter), bf16)], axis=0)
    mix_out = exchange(to_all(jnp.concatenate([w_mix_out, extra], axis=0), tp), "x")

    packed = jnp.stack([dense_gate.T, dense_up.T, dense_down]).reshape(3, tp, slim, quarter)
    packed = jnp.moveaxis(packed, 1, 0).reshape(tp, 3 * slim, quarter)
    dense = exchange(jnp.tile(packed, (far, 1, 1)), FAR + ("x",))
    dense = dense.reshape(far, tp, 3, slim, quarter)
    dense = jnp.transpose(dense, (2, 0, 3, 1, 4)).reshape(3, far * slim, tp * quarter)

    normed_mix = rms_norm(full_tokens, gain_mix)

    def project(weight):
        return dot(normed_mix, weight)

    query_rows = project(w_query).reshape(seqs, -1, HEAD)
    key_rows = project(w_key).reshape(seqs, -1, HEAD) * HEAD ** (-0.5)
    value_rows = project(w_value).reshape(seqs, -1, HEAD)
    out_gate = project(w_outgate)
    input_gate = project(w_input_gate)
    carried = jax.nn.log_sigmoid(project(w_forget_gate)) + max_state
    stabilizer = jnp.maximum(carried, input_gate)
    weight_old = jnp.exp(carried - stabilizer)
    weight_new = jnp.exp(input_gate - stabilizer) * jnp.sum(query_rows * key_rows, axis=-1)
    cell_read = jnp.einsum("bhd,bhde->bhe", query_rows, cell_state, precision=highest)
    numerator = weight_old[..., None] * cell_read + weight_new[..., None] * value_rows
    denominator = weight_old * jnp.sum(query_rows * norm_state, axis=-1) + weight_new
    cell_out = numerator / jnp.maximum(jnp.abs(denominator), 1.0)[..., None]
    mixed = (jax.nn.sigmoid(out_gate) * cell_out.reshape(seqs, -1)).astype(bf16)

    all_heads = side_by_side(exchange(to_all(mixed, tp), "x"))
    width = all_heads.shape[1]
    added = jnp.concatenate([dot(all_heads, mix_out[k, :width]) for k in range(tp)], axis=1)
    resid = (full_tokens.astype(f32) + added).astype(bf16)
    normed = rms_norm(resid, gain_ffn)
    own_resid = lax.dynamic_slice_in_dim(resid, me * quarter, quarter, 1)
    mix_row = mix_out[:, width, :].reshape(1, -1)
    mix_logit = jnp.sum(normed.astype(f32) * mix_row.astype(f32), axis=1, keepdims=True)

    flat_ids = route_ids.reshape(-1)
    picks = (flat_ids[:, None] == jnp.arange(experts, dtype=jnp.int32)[None, :]).astype(bf16)
    chosen = picks.reshape(seqs, TOP, experts).sum(axis=1)
    outgoing = lax.dot_general(chosen, normed, (((0,), (0,)), ((), ())), preferred_element_type=f32)
    received = exchange(outgoing.astype(bf16).reshape(experts, 4, -1), EP)

    group = exchange(to_all(normed, near), NEAR).reshape(near * seqs, -1)

    rows = received.reshape(experts, -1)
    hidden = (jax.nn.silu(dot(rows, expert_gate[0])) * dot(rows, expert_up[0])).astype(bf16)
    partial = dot(hidden, expert_down[0]).astype(bf16)
    returned = exchange(partial.reshape(experts * tp, 2, -1), EP + ("x",))

    transposed = (((1,), (1,)), ((), ()))
    gate_cols = lax.dot_general(group, dense[0], transposed, preferred_element_type=f32)
    up_cols = lax.dot_general(group, dense[1], transposed, preferred_element_type=f32)
    dense_hidden = (jax.nn.silu(gate_cols) * up_cols).astype(bf16)
    dense_part = dot(dense_hidden, dense[2]).astype(bf16)
    dense_part = jnp.transpose(dense_part.reshape(near, seqs, tp, quarter), (0, 2, 1, 3))
    dense_sum = exchange(dense_part.reshape(near * tp, seqs, quarter), NEAR + ("x",))
    dense_out = dense_sum.astype(f32).sum(axis=0)

    result = returned.reshape(experts, tp, quarter).astype(f32).sum(axis=1).astype(bf16)
    picked = dot(picks, result).reshape(seqs, TOP, quarter)
    route_weight = jax.nn.sigmoid(route_logits - route_logits[:, ::-1])
    moe = jnp.sum(route_weight[..., None] * picked, axis=1)
    total = own_resid.astype(f32) + moe + jax.nn.sigmoid(mix_logit) * dense_out
    return total.astype(bf16)


def solution(mesh):
    fine = Mesh(mesh.devices.reshape(4, 2, 4, 2, 2, 4), EP + ("x",))
    return jax.shard_map(
        local,
        mesh=fine,
        in_specs=(
            P(EP, "x"),
            P(),
            P(None, "x"),
            P(None, "x"),
            P(None, "x"),
            P(None, "x"),
            P(None, "x"),
            P(None, "x"),
            P(None, "x"),
            P(EP, "x", None, None),
            P(EP, "x", None),
            P(EP, "x"),
            P(),
            P(EP, None),
            P(EP, None),
            P(EP, None, "x"),
            P(EP, None, "x"),
            P(EP, "x", None),
            P("x", EP),
            P("x", EP),
            P(EP, "x"),
            P("x"),
        ),
        out_specs=P(EP, "x"),
        check_vma=False,
    )
```

```python
import jax
import jax.numpy as jnp
from jax import lax
from jax.sharding import Mesh, PartitionSpec as P

HEAD = 128
TOP = 2
SLOT = 8

epsilon = 1e-06
highest = lax.Precision.HIGHEST
f32 = jnp.float32
bf16 = jnp.bfloat16

FAR = ("zh", "yh")
NEAR = ("zl", "yl", "c")
EP = ("zh", "zl", "yh", "yl", "c")


def exchange(blocks, axis):
    return lax.all_to_all(blocks, axis, 0, 0, tiled=True)


def to_all(shard, size):
    return jnp.broadcast_to(shard[None], (size, *shard.shape))


def side_by_side(blocks):
    count, rows, columns = blocks.shape
    return jnp.moveaxis(blocks, 0, 1).reshape(rows, count * columns)


def rms_norm(rows, gain):
    values = rows.astype(f32)
    scale = lax.rsqrt(jnp.mean(values * values, axis=-1, keepdims=True) + epsilon)
    return (values * scale * gain).astype(bf16)


def dot(a, b):
    return jnp.dot(a, b, preferred_element_type=f32)


def shifted(array, axis, step):
    size = lax.axis_size(axis)
    return lax.ppermute(array, axis, [(i, (i + step) % size) for i in range(size)])


def swapped(array, axis, flip):
    return lax.ppermute(array, axis, [(i, i ^ flip) for i in range(lax.axis_size(axis))])


def layer(
    tokens,
    gain_mix,
    w_query,
    w_key,
    w_value,
    w_outgate,
    w_input_gate,
    w_forget_gate,
    w_mix_out,
    cell_state,
    norm_state,
    max_state,
    gain_ffn,
    route_ids,
    route_logits,
    expert_gate,
    expert_up,
    expert_down,
    dense_gate,
    dense_up,
    dense_down,
    dense_mix,
):
    seqs, quarter = tokens.shape
    tp = lax.axis_size("x")
    far = lax.axis_size(FAR)
    near = lax.axis_size(NEAR)
    experts = lax.axis_size(EP)
    me = lax.axis_index("x")
    place = lax.axis_index(NEAR)
    slim = dense_gate.shape[1] // tp

    packed = jnp.stack([dense_gate.T, dense_up.T, dense_down]).reshape(3, tp, slim, quarter)
    packed = jnp.pad(jnp.moveaxis(packed, 1, 0), ((0, 0), (0, 0), (0, SLOT - slim), (0, 0)))
    packed = packed.reshape(tp, 3 * SLOT, quarter)
    last = jnp.pad(dense_mix[None], ((0, 7), (0, 0)))
    sent = jnp.concatenate([to_all(tokens, tp), packed, to_all(last, tp)], axis=1)
    first = exchange(sent, "x")
    full_tokens = side_by_side(first[:, :seqs])
    mix_row = first[:, seqs + 3 * SLOT].reshape(1, -1)

    mix_out = [w_mix_out]
    for step in (2, 1, 3):
        mix_out.append(shifted(w_mix_out, "x", step))
    mix_out = jnp.stack([mix_out[0], mix_out[2], mix_out[1], mix_out[3]])

    dense = first[None, :, seqs : seqs + 3 * SLOT]
    for axis, flip in (("zh", 2), ("yh", 2), ("zh", 1), ("yh", 1)):
        other = swapped(dense, axis, flip)
        dense = jnp.concatenate([dense, other], axis=0)

    normed_mix = rms_norm(full_tokens, gain_mix)

    def project(weight):
        return dot(normed_mix, weight)

    query_rows = project(w_query).reshape(seqs, -1, HEAD)
    key_rows = project(w_key).reshape(seqs, -1, HEAD) * HEAD ** (-0.5)
    value_rows = project(w_value).reshape(seqs, -1, HEAD)
    out_gate = project(w_outgate)
    input_gate = project(w_input_gate)
    carried = jax.nn.log_sigmoid(project(w_forget_gate)) + max_state
    stabilizer = jnp.maximum(carried, input_gate)
    weight_old = jnp.exp(carried - stabilizer)
    weight_new = jnp.exp(input_gate - stabilizer) * jnp.sum(query_rows * key_rows, axis=-1)
    cell_read = jnp.einsum("bhd,bhde->bhe", query_rows, cell_state, precision=highest)
    numerator = weight_old[..., None] * cell_read + weight_new[..., None] * value_rows
    denominator = weight_old * jnp.sum(query_rows * norm_state, axis=-1) + weight_new
    cell_out = numerator / jnp.maximum(jnp.abs(denominator), 1.0)[..., None]
    mixed = (jax.nn.sigmoid(out_gate) * cell_out.reshape(seqs, -1)).astype(bf16)

    sent = to_all(jnp.concatenate([mixed, tokens], axis=1), near * tp)
    second = exchange(sent, NEAR + ("x",))
    second = second.reshape(near, tp, seqs, HEAD + quarter)
    all_heads = jnp.concatenate(
        [second[:, k, :, :HEAD].reshape(near * seqs, HEAD) for k in range(tp)], axis=1
    )
    resid = []
    for k in range(tp):
        added = dot(all_heads, lax.dynamic_index_in_dim(mix_out, (me - k) % tp, 0, False))
        old = second[:, k, :, HEAD:].reshape(near * seqs, quarter)
        resid.append((old.astype(f32) + added).astype(bf16))
    resid = jnp.concatenate(resid, axis=1)
    group = rms_norm(resid, gain_ffn)
    normed = lax.dynamic_slice_in_dim(group, place * seqs, seqs, 0)
    own_resid = lax.dynamic_slice(resid, (place * seqs, me * quarter), (seqs, quarter))

    flat_ids = route_ids.reshape(-1)
    picks = (flat_ids[:, None] == jnp.arange(experts, dtype=jnp.int32)[None, :]).astype(bf16)
    chosen = picks.reshape(seqs, TOP, experts).sum(axis=1)
    outgoing = lax.dot_general(chosen, normed, (((0,), (0,)), ((), ())), preferred_element_type=f32)
    outgoing = outgoing.astype(bf16).reshape(experts, 4, -1)
    received = exchange(outgoing, EP)

    rows = received.reshape(experts, -1)
    hidden = (jax.nn.silu(dot(rows, expert_gate[0])) * dot(rows, expert_up[0])).astype(bf16)
    partial = dot(hidden, expert_down[0]).astype(bf16).reshape(experts, 4, -1)
    returned = exchange(partial, EP)

    def matrix(place):
        part = dense[:, :, place * SLOT : (place + 1) * SLOT]
        return jnp.moveaxis(part, 1, 2).reshape(far * SLOT, tp * quarter)

    transposed = (((1,), (1,)), ((), ()))
    gate_cols = lax.dot_general(group, matrix(0), transposed, preferred_element_type=f32)
    up_cols = lax.dot_general(group, matrix(1), transposed, preferred_element_type=f32)
    dense_hidden = (jax.nn.silu(gate_cols) * up_cols).astype(bf16)
    dense_part = dot(dense_hidden, matrix(2)).reshape(near, seqs, -1)

    picked = dot(picks, returned.reshape(experts, -1)).reshape(seqs, TOP, -1)
    route_weight = jax.nn.sigmoid(route_logits - route_logits[:, ::-1])
    moe = jnp.sum(route_weight[..., None] * picked, axis=1)
    mix_gate = jax.nn.sigmoid(
        jnp.sum(group.astype(f32) * mix_row.astype(f32), axis=1, keepdims=True)
    ).reshape(near, seqs, 1)
    mine = (jnp.arange(near) == place)[:, None, None]
    part = mix_gate * dense_part + jnp.where(mine, moe[None], 0.0)
    part = jnp.swapaxes(part.astype(bf16).reshape(near, seqs, tp, quarter), 1, 2)
    part = part.reshape(near * tp, seqs, quarter)
    parts = exchange(part, NEAR + ("x",))
    total = own_resid.astype(f32) + parts.astype(f32).sum(axis=0)
    return total.astype(bf16)


def solution(mesh):
    fine = Mesh(mesh.devices.reshape(4, 2, 4, 2, 2, 4), EP + ("x",))
    return jax.shard_map(
        layer,
        mesh=fine,
        in_specs=(
            P(EP, "x"),
            P(),
            P(None, "x"),
            P(None, "x"),
            P(None, "x"),
            P(None, "x"),
            P(None, "x"),
            P(None, "x"),
            P(None, "x"),
            P(EP, "x", None, None),
            P(EP, "x", None),
            P(EP, "x"),
            P(),
            P(EP, None),
            P(EP, None),
            P(EP, None, "x"),
            P(EP, None, "x"),
            P(EP, "x", None),
            P("x", EP),
            P("x", EP),
            P(EP, "x"),
            P("x"),
        ),
        out_specs=P(EP, "x"),
        check_vma=False,
    )
```

```python
import jax
import jax.numpy as jnp
from jax import lax
from jax.sharding import Mesh, PartitionSpec as P

HEAD = 128
TOP = 2

epsilon = 1e-06
highest = lax.Precision.HIGHEST
f32 = jnp.float32
bf16 = jnp.bfloat16

FAR = ("zh", "yh")
NEAR = ("zl", "yl", "c")
EP = ("zh", "zl", "yh", "yl", "c")


def exchange(blocks, axis):
    return lax.all_to_all(blocks, axis, 0, 0, tiled=True)


def to_all(shard, size):
    return jnp.broadcast_to(shard[None], (size, *shard.shape))


def side_by_side(blocks):
    count, rows, columns = blocks.shape
    return jnp.moveaxis(blocks, 0, 1).reshape(rows, count * columns)


def rms_norm(rows, gain):
    values = rows.astype(f32)
    scale = lax.rsqrt(jnp.mean(values * values, axis=-1, keepdims=True) + epsilon)
    return (values * scale * gain).astype(bf16)


def dot(a, b):
    return jnp.dot(a, b, preferred_element_type=f32)


def shifted(array, axis, step):
    size = lax.axis_size(axis)
    return lax.ppermute(array, axis, [(i, (i + step) % size) for i in range(size)])


def layer(
    tokens,
    gain_mix,
    w_query,
    w_key,
    w_value,
    w_outgate,
    w_input_gate,
    w_forget_gate,
    w_mix_out,
    cell_state,
    norm_state,
    max_state,
    gain_ffn,
    route_ids,
    route_logits,
    expert_gate,
    expert_up,
    expert_down,
    dense_gate,
    dense_up,
    dense_down,
    dense_mix,
):
    seqs, quarter = tokens.shape
    tp = lax.axis_size("x")
    far = lax.axis_size(FAR)
    near = lax.axis_size(NEAR)
    experts = lax.axis_size(EP)
    me = lax.axis_index("x")
    place = lax.axis_index(NEAR)
    slim = dense_gate.shape[1] // tp

    packed = jnp.stack([dense_gate.T, dense_up.T, dense_down]).reshape(3, tp, slim, quarter)
    packed = jnp.moveaxis(packed, 1, 0).reshape(tp, 3 * slim, quarter)
    last = jnp.pad(dense_mix[None], ((0, 5), (0, 0)))
    sent = jnp.concatenate([to_all(tokens, tp), packed, to_all(last, tp)], axis=1)
    first = exchange(sent, "x")
    full_tokens = side_by_side(first[:, :seqs])
    mix_row = first[:, seqs + 3 * slim].reshape(1, -1)

    mix_out = [w_mix_out]
    for step in (2, 1, 3):
        mix_out.append(shifted(w_mix_out, "x", step))
    mix_out = jnp.stack([mix_out[0], mix_out[2], mix_out[1], mix_out[3]])

    dense = to_all(first[:, seqs : seqs + 3 * slim].reshape(tp * 3 * slim, quarter), far)
    dense = exchange(dense, FAR)
    dense = jnp.transpose(dense.reshape(far, tp, 3, slim, quarter), (2, 0, 3, 1, 4))
    dense = dense.reshape(3, far * slim, tp * quarter)

    normed_mix = rms_norm(full_tokens, gain_mix)

    def project(weight):
        return dot(normed_mix, weight)

    query_rows = project(w_query).reshape(seqs, -1, HEAD)
    key_rows = project(w_key).reshape(seqs, -1, HEAD) * HEAD ** (-0.5)
    value_rows = project(w_value).reshape(seqs, -1, HEAD)
    out_gate = project(w_outgate)
    input_gate = project(w_input_gate)
    carried = jax.nn.log_sigmoid(project(w_forget_gate)) + max_state
    stabilizer = jnp.maximum(carried, input_gate)
    weight_old = jnp.exp(carried - stabilizer)
    weight_new = jnp.exp(input_gate - stabilizer) * jnp.sum(query_rows * key_rows, axis=-1)
    cell_read = jnp.einsum("bhd,bhde->bhe", query_rows, cell_state, precision=highest)
    numerator = weight_old[..., None] * cell_read + weight_new[..., None] * value_rows
    denominator = weight_old * jnp.sum(query_rows * norm_state, axis=-1) + weight_new
    cell_out = numerator / jnp.maximum(jnp.abs(denominator), 1.0)[..., None]
    mixed = (jax.nn.sigmoid(out_gate) * cell_out.reshape(seqs, -1)).astype(bf16)

    sent = to_all(jnp.concatenate([mixed, tokens], axis=1), near * tp)
    second = exchange(sent, NEAR + ("x",))
    second = second.reshape(near, tp, seqs, HEAD + quarter)
    all_heads = jnp.concatenate(
        [second[:, k, :, :HEAD].reshape(near * seqs, HEAD) for k in range(tp)], axis=1
    )
    resid = []
    for k in range(tp):
        added = dot(all_heads, lax.dynamic_index_in_dim(mix_out, (me - k) % tp, 0, False))
        old = second[:, k, :, HEAD:].reshape(near * seqs, quarter)
        resid.append((old.astype(f32) + added).astype(bf16))
    resid = jnp.concatenate(resid, axis=1)
    group = rms_norm(resid, gain_ffn)
    normed = lax.dynamic_slice_in_dim(group, place * seqs, seqs, 0)
    own_resid = lax.dynamic_slice(resid, (place * seqs, me * quarter), (seqs, quarter))

    flat_ids = route_ids.reshape(-1)
    picks = (flat_ids[:, None] == jnp.arange(experts, dtype=jnp.int32)[None, :]).astype(bf16)
    chosen = picks.reshape(seqs, TOP, experts).sum(axis=1)
    outgoing = lax.dot_general(chosen, normed, (((0,), (0,)), ((), ())), preferred_element_type=f32)
    outgoing = outgoing.astype(bf16).reshape(experts, 4, -1)
    received = exchange(outgoing, EP)

    rows = received.reshape(experts, -1)
    hidden = (jax.nn.silu(dot(rows, expert_gate[0])) * dot(rows, expert_up[0])).astype(bf16)
    partial = dot(hidden, expert_down[0]).astype(bf16).reshape(experts, 4, -1)
    returned = exchange(partial, EP)

    transposed = (((1,), (1,)), ((), ()))
    gate_cols = lax.dot_general(group, dense[0], transposed, preferred_element_type=f32)
    up_cols = lax.dot_general(group, dense[1], transposed, preferred_element_type=f32)
    dense_hidden = (jax.nn.silu(gate_cols) * up_cols).astype(bf16)
    dense_part = dot(dense_hidden, dense[2]).reshape(near, seqs, -1)

    picked = dot(picks, returned.reshape(experts, -1)).reshape(seqs, TOP, -1)
    route_weight = jax.nn.sigmoid(route_logits - route_logits[:, ::-1])
    moe = jnp.sum(route_weight[..., None] * picked, axis=1)
    mix_gate = jax.nn.sigmoid(
        jnp.sum(group.astype(f32) * mix_row.astype(f32), axis=1, keepdims=True)
    ).reshape(near, seqs, 1)
    mine = (jnp.arange(near) == place)[:, None, None]
    part = mix_gate * dense_part + jnp.where(mine, moe[None], 0.0)
    part = jnp.swapaxes(part.astype(bf16).reshape(near, seqs, tp, quarter), 1, 2)
    part = part.reshape(near * tp, seqs, quarter)
    parts = exchange(part, NEAR + ("x",))
    total = own_resid.astype(f32) + parts.astype(f32).sum(axis=0)
    return total.astype(bf16)


def solution(mesh):
    fine = Mesh(mesh.devices.reshape(4, 2, 4, 2, 2, 4), EP + ("x",))
    return jax.shard_map(
        layer,
        mesh=fine,
        in_specs=(
            P(EP, "x"),
            P(),
            P(None, "x"),
            P(None, "x"),
            P(None, "x"),
            P(None, "x"),
            P(None, "x"),
            P(None, "x"),
            P(None, "x"),
            P(EP, "x", None, None),
            P(EP, "x", None),
            P(EP, "x"),
            P(),
            P(EP, None),
            P(EP, None),
            P(EP, None, "x"),
            P(EP, None, "x"),
            P(EP, "x", None),
            P("x", EP),
            P("x", EP),
            P(EP, "x"),
            P("x"),
        ),
        out_specs=P(EP, "x"),
        check_vma=False,
    )
```

```python
import jax
import jax.numpy as jnp
from jax import lax
from jax.sharding import Mesh, PartitionSpec as P

HEAD = 128
TOP = 2

epsilon = 1e-06
highest = lax.Precision.HIGHEST
f32 = jnp.float32
bf16 = jnp.bfloat16

FAR = ("zh", "yh")
NEAR = ("zl", "yl", "c")
EP = ("zh", "zl", "yh", "yl", "c")


def exchange(blocks, axis):
    return lax.all_to_all(blocks, axis, 0, 0, tiled=True)


def to_all(shard, size):
    return jnp.broadcast_to(shard[None], (size, *shard.shape))


def side_by_side(blocks):
    count, rows, columns = blocks.shape
    return jnp.moveaxis(blocks, 0, 1).reshape(rows, count * columns)


def rms_norm(rows, gain):
    values = rows.astype(f32)
    scale = lax.rsqrt(jnp.mean(values * values, axis=-1, keepdims=True) + epsilon)
    return (values * scale * gain).astype(bf16)


def dot(a, b):
    return jnp.dot(a, b, preferred_element_type=f32)


def shifted(array, axis, step):
    size = lax.axis_size(axis)
    return lax.ppermute(array, axis, [(i, (i + step) % size) for i in range(size)])


def layer(
    tokens,
    gain_mix,
    w_query,
    w_key,
    w_value,
    w_outgate,
    w_input_gate,
    w_forget_gate,
    w_mix_out,
    cell_state,
    norm_state,
    max_state,
    gain_ffn,
    route_ids,
    route_logits,
    expert_gate,
    expert_up,
    expert_down,
    dense_gate,
    dense_up,
    dense_down,
    dense_mix,
):
    seqs, quarter = tokens.shape
    tp = lax.axis_size("x")
    far = lax.axis_size(FAR)
    near = lax.axis_size(NEAR)
    experts = lax.axis_size(EP)
    me = lax.axis_index("x")
    place = lax.axis_index(NEAR)
    slim = dense_gate.shape[1] // tp

    packed = jnp.stack([dense_gate.T, dense_up.T, dense_down]).reshape(3, tp, slim, quarter)
    packed = jnp.moveaxis(packed, 1, 0).reshape(tp, 3 * slim, quarter)
    last = jnp.pad(dense_mix[None], ((0, 5), (0, 0)))
    sent = jnp.concatenate([to_all(tokens, tp), packed, to_all(last, tp)], axis=1)
    first = exchange(sent, "x")
    full_tokens = side_by_side(first[:, :seqs])
    mix_row = first[:, seqs + 3 * slim].reshape(1, -1)

    mix_out = {0: w_mix_out}
    for step in (2, 1, 3):
        mix_out[step] = shifted(w_mix_out, "x", step)

    dense = to_all(first[:, seqs : seqs + 3 * slim].reshape(tp * 3 * slim, quarter), far)
    dense = exchange(dense, FAR)
    dense = jnp.transpose(dense.reshape(far, tp, 3, slim, quarter), (2, 0, 3, 1, 4))
    dense = dense.reshape(3, far * slim, tp * quarter)

    normed_mix = rms_norm(full_tokens, gain_mix)

    def project(weight):
        return dot(normed_mix, weight)

    query_rows = project(w_query).reshape(seqs, -1, HEAD)
    key_rows = project(w_key).reshape(seqs, -1, HEAD) * HEAD ** (-0.5)
    value_rows = project(w_value).reshape(seqs, -1, HEAD)
    out_gate = project(w_outgate)
    input_gate = project(w_input_gate)
    carried = jax.nn.log_sigmoid(project(w_forget_gate)) + max_state
    stabilizer = jnp.maximum(carried, input_gate)
    weight_old = jnp.exp(carried - stabilizer)
    weight_new = jnp.exp(input_gate - stabilizer) * jnp.sum(query_rows * key_rows, axis=-1)
    cell_read = jnp.einsum("bhd,bhde->bhe", query_rows, cell_state, precision=highest)
    numerator = weight_old[..., None] * cell_read + weight_new[..., None] * value_rows
    denominator = weight_old * jnp.sum(query_rows * norm_state, axis=-1) + weight_new
    cell_out = numerator / jnp.maximum(jnp.abs(denominator), 1.0)[..., None]
    mixed = (jax.nn.sigmoid(out_gate) * cell_out.reshape(seqs, -1)).astype(bf16)

    sent = to_all(mixed, tp)
    second = exchange(sent, "x")
    all_heads = side_by_side(second)
    added = jnp.stack([dot(all_heads, mix_out[k]) for k in range(tp)])
    added = [lax.dynamic_index_in_dim(added, (me - k) & (tp - 1), 0, False) for k in range(tp)]
    resid = (full_tokens.astype(f32) + jnp.concatenate(added, axis=1)).astype(bf16)
    normed = rms_norm(resid, gain_ffn)
    own_resid = lax.dynamic_slice_in_dim(resid, me * quarter, quarter, 1)

    flat_ids = route_ids.reshape(-1)
    picks = (flat_ids[:, None] == jnp.arange(experts, dtype=jnp.int32)[None, :]).astype(bf16)
    chosen = picks.reshape(seqs, TOP, experts).sum(axis=1)
    outgoing = lax.dot_general(chosen, normed, (((0,), (0,)), ((), ())), preferred_element_type=f32)
    outgoing = outgoing.astype(bf16).reshape(experts, 4, -1)
    received = exchange(outgoing, EP)

    group = normed
    for axis in ("c", "yl", "zl"):
        other = lax.ppermute(group, axis, [(0, 1), (1, 0)])
        low = lax.axis_index(axis) == 0
        group = jnp.concatenate(
            [jnp.where(low, group, other), jnp.where(low, other, group)], axis=0
        )

    rows = received.reshape(experts, -1)
    hidden = (jax.nn.silu(dot(rows, expert_gate[0])) * dot(rows, expert_up[0])).astype(bf16)
    partial = dot(hidden, expert_down[0]).astype(bf16).reshape(experts, 4, -1)
    returned = exchange(partial, EP)

    transposed = (((1,), (1,)), ((), ()))
    gate_cols = lax.dot_general(group, dense[0], transposed, preferred_element_type=f32)
    up_cols = lax.dot_general(group, dense[1], transposed, preferred_element_type=f32)
    dense_hidden = (jax.nn.silu(gate_cols) * up_cols).astype(bf16)
    dense_part = dot(dense_hidden, dense[2]).reshape(near, seqs, -1)

    picked = dot(picks, returned.reshape(experts, -1)).reshape(seqs, TOP, -1)
    route_weight = jax.nn.sigmoid(route_logits - route_logits[:, ::-1])
    moe = jnp.sum(route_weight[..., None] * picked, axis=1)
    mix_gate = jax.nn.sigmoid(
        jnp.sum(group.astype(f32) * mix_row.astype(f32), axis=1, keepdims=True)
    ).reshape(near, seqs, 1)
    mine = (jnp.arange(near) == place)[:, None, None]
    part = mix_gate * dense_part + jnp.where(mine, moe[None], 0.0)
    part = jnp.swapaxes(part.astype(bf16).reshape(near, seqs, tp, quarter), 1, 2)
    part = part.reshape(near * tp, seqs, quarter)
    parts = exchange(part, NEAR + ("x",))
    total = own_resid.astype(f32) + parts.astype(f32).sum(axis=0)
    return total.astype(bf16)


def solution(mesh):
    fine = Mesh(mesh.devices.reshape(4, 2, 4, 2, 2, 4), EP + ("x",))
    return jax.shard_map(
        layer,
        mesh=fine,
        in_specs=(
            P(EP, "x"),
            P(),
            P(None, "x"),
            P(None, "x"),
            P(None, "x"),
            P(None, "x"),
            P(None, "x"),
            P(None, "x"),
            P(None, "x"),
            P(EP, "x", None, None),
            P(EP, "x", None),
            P(EP, "x"),
            P(),
            P(EP, None),
            P(EP, None),
            P(EP, None, "x"),
            P(EP, None, "x"),
            P(EP, "x", None),
            P("x", EP),
            P("x", EP),
            P(EP, "x"),
            P("x"),
        ),
        out_specs=P(EP, "x"),
        check_vma=False,
    )
```

```python
import jax
import jax.numpy as jnp
from jax import lax
from jax.experimental import pallas as pl
from jax.experimental.pallas import tpu as pltpu
from jax.sharding import Mesh, PartitionSpec as P

HEAD = 128
TOP = 2

epsilon = 1e-06
f32 = jnp.float32
bf16 = jnp.bfloat16

FAR = ("zh", "yh")
NEAR = ("zl", "yl", "c")
EP = ("zh", "zl", "yh", "yl", "c")


def exchange(blocks, axis):
    return lax.all_to_all(blocks, axis, 0, 0, tiled=True)


def to_all(shard, size):
    return jnp.broadcast_to(shard[None], (size, *shard.shape))


def dot(a, b):
    return jnp.dot(a, b, preferred_element_type=f32)


def shifted(array, axis, step):
    size = lax.axis_size(axis)
    return lax.ppermute(array, axis, [(i, (i + step) % size) for i in range(size)])


def pack_kernel(tokens, gate, up, down, mix, out):
    seqs, quarter = tokens.shape
    count, columns = out.shape[0], gate.shape[0]
    slim = columns // count
    room = out.shape[1] - seqs
    source = jnp.concatenate([gate[...], up[...], down[...]], axis=0)
    row = lax.broadcasted_iota(jnp.int32, (room, 3 * columns), 0)
    column = lax.broadcasted_iota(jnp.int32, (room, 3 * columns), 1)
    wanted = jnp.where(
        row < slim,
        row,
        jnp.where(row < 2 * slim, row + columns - slim, row + 2 * (columns - slim)),
    )
    last = lax.broadcasted_iota(jnp.int32, (room, quarter), 0) == 3 * slim
    extra = jnp.where(last, jnp.broadcast_to(mix[...].astype(f32), (room, quarter)), 0.0)
    for k in range(count):
        pick = ((column == wanted + k * slim) & (row < 3 * slim)).astype(f32).astype(bf16)
        out[k, :seqs] = tokens[...]
        out[k, seqs:] = (dot(pick, source) + extra).astype(bf16)


def pack(tokens, gate, up, down, mix, count):
    seqs, quarter = tokens.shape
    slim = gate.shape[0] // count
    rows = -(-(seqs + 3 * slim + 1) // 8) * 8
    return pl.pallas_call(
        pack_kernel,
        out_shape=jax.ShapeDtypeStruct((count, rows, quarter), bf16),
        name="pack",
    )(tokens, gate, up, down, mix)


def cell_kernel(first, gain, wq, wk, wv, wo, wi, wf, state, norm, peak, out):
    seqs = norm.shape[0]
    values = jnp.concatenate([first[k, :seqs] for k in range(first.shape[0])], axis=1).astype(f32)
    scale = lax.rsqrt(jnp.mean(values * values, axis=1, keepdims=True) + epsilon)
    rows = (values * scale * gain[...]).astype(bf16)
    query = dot(rows, wq[...])
    key = dot(rows, wk[...]) * HEAD ** (-0.5)
    value = dot(rows, wv[...])
    gate = jax.nn.sigmoid(dot(rows, wo[...]))
    wide = rows.astype(f32)
    enter = jnp.sum(wide * wi[...].astype(f32), axis=1, keepdims=True)
    forget = jnp.sum(wide * wf[...].astype(f32), axis=1, keepdims=True)
    carried = jnp.minimum(forget, 0.0) - jnp.log1p(jnp.exp(-jnp.abs(forget))) + peak[...]
    stabilizer = jnp.maximum(carried, enter)
    old = jnp.exp(carried - stabilizer)
    new = jnp.exp(enter - stabilizer) * jnp.sum(query * key, axis=1, keepdims=True)
    turned = query.T
    read = [
        jnp.sum(turned[:, b : b + 1] * state[b], axis=0, keepdims=True) for b in range(seqs)
    ]
    numerator = old * jnp.concatenate(read, axis=0) + new * value
    denominator = old * jnp.sum(query * norm[...], axis=1, keepdims=True) + new
    mixed = gate * (numerator / jnp.maximum(jnp.abs(denominator), 1.0))
    for k in range(out.shape[0]):
        out[k] = mixed.astype(bf16)


def cell(first, gain, wq, wk, wv, wo, wi, wf, state, norm, peak):
    return pl.pallas_call(
        cell_kernel,
        out_shape=jax.ShapeDtypeStruct((1, *norm.shape), bf16),
        cost_estimate=pl.CostEstimate(flops=40000000, bytes_accessed=2200000, transcendentals=9000),
        compiler_params=pltpu.CompilerParams(vmem_limit_bytes=12 << 20),
        name="cell",
    )(first, gain, wq, wk, wv, wo, wi, wf, state, norm, peak)


def residual_kernel(me, place, second, w0, w1, w2, w3, gain, ids, group, outgoing, own, resid):
    near, tp, seqs, _ = second.shape
    quarter = w0.shape[1]
    heads = jnp.concatenate(
        [
            jnp.concatenate([second[s, k, :, :HEAD] for s in range(near)], axis=0)
            for k in range(tp)
        ],
        axis=1,
    )
    total = jnp.zeros((near * seqs, 1), f32)
    for step, weight in enumerate((w0, w1, w2, w3)):
        k = (me[0] + tp - step) & (tp - 1)
        added = dot(heads, weight[...])
        old = jnp.concatenate([second[s, k, :, HEAD:] for s in range(near)], axis=0)
        values = (old.astype(f32) + added).astype(bf16)
        wide = values.astype(f32)
        total = total + jnp.sum(wide * wide, axis=1, keepdims=True)
        resid[:, pl.ds(pl.multiple_of(k * quarter, quarter), quarter)] = wide
        if step == 0:
            group[:, :quarter] = values
    start = pl.multiple_of(place[0] * seqs, seqs)
    own[...] = group[pl.ds(start, seqs), :quarter]
    scale = lax.rsqrt(total * (1.0 / (tp * quarter)) + epsilon)
    group[...] = (resid[...] * scale * gain[...]).astype(bf16)
    experts = outgoing.shape[0]
    expert = lax.broadcasted_iota(jnp.int32, (experts, seqs), 0)
    chosen = ((expert == ids[0:1, :]) | (expert == ids[1:2, :])).astype(f32).astype(bf16)
    outgoing[...] = dot(chosen, group[pl.ds(start, seqs), :]).astype(bf16)


def residual(me, place, second, weights, gain, ids, experts):
    near, tp, seqs, _ = second.shape
    quarter = weights[0].shape[1]
    whole = pl.BlockSpec(memory_space=pltpu.VMEM)
    scalar = pl.BlockSpec(memory_space=pltpu.SMEM)
    return pl.pallas_call(
        residual_kernel,
        out_shape=(
            jax.ShapeDtypeStruct((near * seqs, tp * quarter), bf16),
            jax.ShapeDtypeStruct((experts, tp * quarter), bf16),
            jax.ShapeDtypeStruct((seqs, quarter), bf16),
        ),
        in_specs=[scalar, scalar] + [whole] * 7,
        out_specs=(whole, whole, whole),
        scratch_shapes=[pltpu.VMEM((near * seqs, tp * quarter), f32)],
        cost_estimate=pl.CostEstimate(flops=140000000, bytes_accessed=2000000, transcendentals=128),
        compiler_params=pltpu.CompilerParams(vmem_limit_bytes=12 << 20),
        name="residual",
    )(me[None], place[None], second, *weights, gain, ids)


def layer(
    tokens,
    gain_mix,
    w_query,
    w_key,
    w_value,
    w_outgate,
    w_input_gate,
    w_forget_gate,
    w_mix_out,
    cell_state,
    norm_state,
    max_state,
    gain_ffn,
    route_ids,
    route_logits,
    expert_gate,
    expert_up,
    expert_down,
    dense_gate,
    dense_up,
    dense_down,
    dense_mix,
):
    seqs, quarter = tokens.shape
    tp = lax.axis_size("x")
    far = lax.axis_size(FAR)
    near = lax.axis_size(NEAR)
    experts = lax.axis_size(EP)
    me = lax.axis_index("x")
    place = lax.axis_index(NEAR)
    slim = dense_gate.shape[1] // tp

    sent = pack(tokens, dense_gate.T, dense_up.T, dense_down, dense_mix[None], tp)
    first = exchange(sent, "x")
    mix_row = first[:, seqs + 3 * slim].reshape(1, -1)

    mix_out = {0: w_mix_out}
    for step in (2, 1, 3):
        mix_out[step] = shifted(w_mix_out, "x", step)

    dense = to_all(first[:, seqs : seqs + 3 * slim].reshape(tp * 3 * slim, quarter), far)
    dense = exchange(dense, FAR)
    dense = jnp.transpose(dense.reshape(far, tp, 3, slim, quarter), (2, 0, 3, 1, 4))
    dense = dense.reshape(3, far * slim, tp * quarter)

    mixed = cell(
        first,
        gain_mix[None],
        w_query,
        w_key,
        w_value,
        w_outgate,
        w_input_gate.T,
        w_forget_gate.T,
        cell_state[:, 0],
        norm_state[:, 0],
        max_state,
    )[0]
    sent = to_all(jnp.concatenate([mixed, tokens], axis=1), near * tp)
    second = exchange(sent, NEAR + ("x",))
    second = second.reshape(near, tp, seqs, HEAD + quarter)
    group, outgoing, own_resid = residual(
        me, place, second, [mix_out[k] for k in range(tp)], gain_ffn[None], route_ids.T, experts
    )

    flat_ids = route_ids.reshape(-1)
    picks = (flat_ids[:, None] == jnp.arange(experts, dtype=jnp.int32)[None, :]).astype(bf16)
    outgoing = outgoing.reshape(experts, 4, -1)
    received = exchange(outgoing, EP)

    rows = received.reshape(experts, -1)
    hidden = (jax.nn.silu(dot(rows, expert_gate[0])) * dot(rows, expert_up[0])).astype(bf16)
    partial = dot(hidden, expert_down[0]).astype(bf16).reshape(experts, 4, -1)
    returned = exchange(partial, EP)

    transposed = (((1,), (1,)), ((), ()))
    gate_cols = lax.dot_general(group, dense[0], transposed, preferred_element_type=f32)
    up_cols = lax.dot_general(group, dense[1], transposed, preferred_element_type=f32)
    dense_hidden = (jax.nn.silu(gate_cols) * up_cols).astype(bf16)
    dense_part = dot(dense_hidden, dense[2]).reshape(near, seqs, -1)

    picked = dot(picks, returned.reshape(experts, -1)).reshape(seqs, TOP, -1)
    route_weight = jax.nn.sigmoid(route_logits - route_logits[:, ::-1])
    moe = jnp.sum(route_weight[..., None] * picked, axis=1)
    mix_gate = jax.nn.sigmoid(
        jnp.sum(group.astype(f32) * mix_row.astype(f32), axis=1, keepdims=True)
    ).reshape(near, seqs, 1)
    mine = (jnp.arange(near) == place)[:, None, None]
    part = mix_gate * dense_part + jnp.where(mine, moe[None], 0.0)
    part = jnp.swapaxes(part.astype(bf16).reshape(near, seqs, tp, quarter), 1, 2)
    part = part.reshape(near * tp, seqs, quarter)
    parts = exchange(part, NEAR + ("x",))
    total = own_resid.astype(f32) + parts.astype(f32).sum(axis=0)
    return total.astype(bf16)


def solution(mesh):
    fine = Mesh(mesh.devices.reshape(4, 2, 4, 2, 2, 4), EP + ("x",))
    return jax.shard_map(
        layer,
        mesh=fine,
        in_specs=(
            P(EP, "x"),
            P(),
            P(None, "x"),
            P(None, "x"),
            P(None, "x"),
            P(None, "x"),
            P(None, "x"),
            P(None, "x"),
            P(None, "x"),
            P(EP, "x", None, None),
            P(EP, "x", None),
            P(EP, "x"),
            P(),
            P(EP, None),
            P(EP, None),
            P(EP, None, "x"),
            P(EP, None, "x"),
            P(EP, "x", None),
            P("x", EP),
            P("x", EP),
            P(EP, "x"),
            P("x"),
        ),
        out_specs=P(EP, "x"),
        check_vma=False,
    )
```

```python
import jax
import jax.numpy as jnp
from jax import lax
from jax.experimental import pallas as pl
from jax.experimental.pallas import tpu as pltpu
from jax.sharding import Mesh, PartitionSpec as P

HEAD = 128

epsilon = 1e-06
f32 = jnp.float32
bf16 = jnp.bfloat16

FAR = ("zh", "yh", "c")
NEAR = ("zl", "yl")
SLOT = 8
EP = ("zh", "zl", "yh", "yl", "c")


def exchange(blocks, axis):
    return lax.all_to_all(blocks, axis, 0, 0, tiled=True)


def to_all(shard, size):
    return jnp.broadcast_to(shard[None], (size, *shard.shape))


def dot(a, b):
    return jnp.dot(a, b, preferred_element_type=f32)


def dot_turned(a, b):
    return lax.dot_general(a, b, (((1,), (1,)), ((), ())), preferred_element_type=f32)


def shifted(array, axis, step):
    size = lax.axis_size(axis)
    return lax.ppermute(array, axis, [(i, (i + step) % size) for i in range(size)])


def pack_kernel(tokens, gate, up, down, mix, out):
    seqs, quarter = tokens.shape
    count, columns = out.shape[0], gate.shape[0]
    slim = columns // count
    room = out.shape[1] - seqs
    source = jnp.concatenate([gate[...], up[...], down[...]], axis=0)
    row = lax.broadcasted_iota(jnp.int32, (room, 3 * columns), 0)
    column = lax.broadcasted_iota(jnp.int32, (room, 3 * columns), 1)
    slot = row & (SLOT - 1)
    wanted = slot + lax.div(row, SLOT) * columns
    last = lax.broadcasted_iota(jnp.int32, (room, quarter), 0) == 3 * SLOT
    extra = jnp.where(last, jnp.broadcast_to(mix[...].astype(f32), (room, quarter)), 0.0)
    for k in range(count):
        pick = (column == wanted + k * slim) & (slot < slim) & (row < 3 * SLOT)
        out[k, :seqs] = tokens[...]
        out[k, seqs:] = (dot(pick.astype(f32).astype(bf16), source) + extra).astype(bf16)


def pack(tokens, gate, up, down, mix, count):
    seqs, quarter = tokens.shape
    return pl.pallas_call(
        pack_kernel,
        out_shape=jax.ShapeDtypeStruct((count, seqs + 4 * SLOT, quarter), bf16),
        name="pack",
    )(tokens, gate, up, down, mix)


def cell_kernel(first, gain, wq, wk, wv, wo, wi, wf, state, norm, peak, out):
    seqs = norm.shape[0]
    values = jnp.concatenate([first[k, :seqs] for k in range(first.shape[0])], axis=1).astype(f32)
    scale = lax.rsqrt(jnp.mean(values * values, axis=1, keepdims=True) + epsilon)
    rows = (values * scale * gain[...]).astype(bf16)
    query = dot(rows, wq[...])
    key = dot(rows, wk[...]) * HEAD ** (-0.5)
    value = dot(rows, wv[...])
    gate = jax.nn.sigmoid(dot(rows, wo[...]))
    wide = rows.astype(f32)
    enter = jnp.sum(wide * wi[...].astype(f32), axis=1, keepdims=True)
    forget = jnp.sum(wide * wf[...].astype(f32), axis=1, keepdims=True)
    carried = jnp.minimum(forget, 0.0) - jnp.log1p(jnp.exp(-jnp.abs(forget))) + peak[...]
    stabilizer = jnp.maximum(carried, enter)
    old = jnp.exp(carried - stabilizer)
    new = jnp.exp(enter - stabilizer) * jnp.sum(query * key, axis=1, keepdims=True)
    turned = query.T
    read = [
        jnp.sum(turned[:, b : b + 1] * state[b], axis=0, keepdims=True) for b in range(seqs)
    ]
    numerator = old * jnp.concatenate(read, axis=0) + new * value
    denominator = old * jnp.sum(query * norm[...], axis=1, keepdims=True) + new
    mixed = gate * (numerator / jnp.maximum(jnp.abs(denominator), 1.0))
    for k in range(out.shape[0]):
        out[k] = mixed.astype(bf16)


def cell(first, gain, wq, wk, wv, wo, wi, wf, state, norm, peak):
    return pl.pallas_call(
        cell_kernel,
        out_shape=jax.ShapeDtypeStruct((1, *norm.shape), bf16),
        cost_estimate=pl.CostEstimate(flops=40000000, bytes_accessed=2200000, transcendentals=9000),
        name="cell",
    )(first, gain, wq, wk, wv, wo, wi, wf, state, norm, peak)


def residual_kernel(me, place, second, w0, w1, w2, w3, gain, ids, group, outgoing, own, resid):
    near, tp, seqs, _ = second.shape
    quarter = w0.shape[1]
    heads = jnp.concatenate(
        [
            jnp.concatenate([second[s, k, :, :HEAD] for s in range(near)], axis=0)
            for k in range(tp)
        ],
        axis=1,
    )
    total = jnp.zeros((near * seqs, 1), f32)
    for step, weight in enumerate((w0, w1, w2, w3)):
        k = (me[0] + tp - step) & (tp - 1)
        added = dot(heads, weight[...])
        old = jnp.concatenate([second[s, k, :, HEAD:] for s in range(near)], axis=0)
        values = (old.astype(f32) + added).astype(bf16)
        wide = values.astype(f32)
        total = total + jnp.sum(wide * wide, axis=1, keepdims=True)
        resid[:, pl.ds(pl.multiple_of(k * quarter, quarter), quarter)] = wide
        if step == 0:
            group[:, :quarter] = values
    start = pl.multiple_of(place[0] * seqs, seqs)
    own[...] = group[pl.ds(start, seqs), :quarter]
    scale = lax.rsqrt(total * (1.0 / (tp * quarter)) + epsilon)
    group[...] = (resid[...] * scale * gain[...]).astype(bf16)
    experts = outgoing.shape[0]
    expert = lax.broadcasted_iota(jnp.int32, (experts, seqs), 0)
    chosen = ((expert == ids[0:1, :]) | (expert == ids[1:2, :])).astype(f32).astype(bf16)
    outgoing[...] = dot(chosen, group[pl.ds(start, seqs), :]).astype(bf16)


def residual(me, place, second, weights, gain, ids, experts):
    near, tp, seqs, _ = second.shape
    quarter = weights[0].shape[1]
    whole = pl.BlockSpec(memory_space=pltpu.VMEM)
    scalar = pl.BlockSpec(memory_space=pltpu.SMEM)
    return pl.pallas_call(
        residual_kernel,
        out_shape=(
            jax.ShapeDtypeStruct((near * seqs, tp * quarter), bf16),
            jax.ShapeDtypeStruct((experts, tp * quarter), bf16),
            jax.ShapeDtypeStruct((seqs, quarter), bf16),
        ),
        in_specs=[scalar, scalar] + [whole] * 7,
        out_specs=(whole, whole, whole),
        scratch_shapes=[pltpu.VMEM((near * seqs, tp * quarter), f32)],
        cost_estimate=pl.CostEstimate(flops=140000000, bytes_accessed=2000000, transcendentals=128),
        compiler_params=pltpu.CompilerParams(vmem_limit_bytes=12 << 20),
        name="residual",
    )(me[None], place[None], second, *weights, gain, ids)


def dense_kernel(group, weights, mix, out):
    far, tp, _, quarter = weights.shape

    def matrix(k, place):
        return weights[:, k, place * SLOT : (place + 1) * SLOT].reshape(far * SLOT, quarter)

    rows = group[...]
    gate, up = 0.0, 0.0
    for k in range(tp):
        part = rows[:, k * quarter : (k + 1) * quarter]
        gate = gate + dot_turned(part, matrix(k, 0))
        up = up + dot_turned(part, matrix(k, 1))
    hidden = (gate * jax.nn.sigmoid(gate) * up).astype(bf16)
    logit = jnp.sum(rows.astype(f32) * mix[...].astype(f32), axis=1, keepdims=True)
    mix_gate = jax.nn.sigmoid(logit)
    for k in range(tp):
        out[:, k * quarter : (k + 1) * quarter] = mix_gate * dot(hidden, matrix(k, 2))


def dense_branch(group, weights, mix):
    return pl.pallas_call(
        dense_kernel,
        out_shape=jax.ShapeDtypeStruct(group.shape, f32),
        compiler_params=pltpu.CompilerParams(vmem_limit_bytes=12 << 20),
        cost_estimate=pl.CostEstimate(flops=100000000, bytes_accessed=1800000, transcendentals=32000),
        name="dense",
    )(group, weights, mix)


def combine_kernel(place, part, returned, ids, weights, out):
    seqs, quarter = out.shape[1:]
    experts = returned.shape[0]
    tp = returned.shape[1] // quarter
    expert = lax.broadcasted_iota(jnp.int32, (seqs, experts), 1)
    here = ids[...]
    weight = weights[...]
    rows = returned[...]
    first = dot((expert == here[:, 0:1]).astype(f32).astype(bf16), rows)
    second = dot((expert == here[:, 1:2]).astype(f32).astype(bf16), rows)
    moe = weight[:, 0:1] * first + weight[:, 1:2] * second
    for s in range(out.shape[0] // tp):
        mine = jnp.where(place[0] == s, 1.0, 0.0)
        for k in range(tp):
            columns = slice(k * quarter, (k + 1) * quarter)
            value = part[s * seqs : (s + 1) * seqs, columns] + mine * moe[:, columns]
            out[s * tp + k] = value.astype(bf16)


def combine(place, part, returned, ids, weights, quarter):
    seqs = ids.shape[0]
    whole = pl.BlockSpec(memory_space=pltpu.VMEM)
    count = part.shape[0] // seqs * (part.shape[1] // quarter)
    return pl.pallas_call(
        combine_kernel,
        out_shape=jax.ShapeDtypeStruct((count, seqs, quarter), bf16),
        in_specs=[pl.BlockSpec(memory_space=pltpu.SMEM)] + [whole] * 4,
        out_specs=whole,
        compiler_params=pltpu.CompilerParams(vmem_limit_bytes=8 << 20),
        name="combine",
    )(place[None], part, returned, ids, weights)


def layer(
    tokens,
    gain_mix,
    w_query,
    w_key,
    w_value,
    w_outgate,
    w_input_gate,
    w_forget_gate,
    w_mix_out,
    cell_state,
    norm_state,
    max_state,
    gain_ffn,
    route_ids,
    route_logits,
    expert_gate,
    expert_up,
    expert_down,
    dense_gate,
    dense_up,
    dense_down,
    dense_mix,
):
    seqs, quarter = tokens.shape
    tp = lax.axis_size("x")
    far = lax.axis_size(FAR)
    near = lax.axis_size(NEAR)
    experts = lax.axis_size(EP)
    me = lax.axis_index("x")
    place = lax.axis_index(NEAR)

    sent = pack(tokens, dense_gate.T, dense_up.T, dense_down, dense_mix[None], tp)
    first = exchange(sent, "x")
    mix_row = first[:, seqs + 3 * SLOT].reshape(1, -1)

    route_weight = jax.nn.sigmoid(route_logits - route_logits[:, ::-1])

    mix_out = {0: w_mix_out}
    for step in (2, 1, 3):
        mix_out[step] = shifted(w_mix_out, "x", step)

    dense = lax.all_gather(first[:, seqs : seqs + 3 * SLOT].reshape(-1, quarter), FAR)
    dense = dense.reshape(far, tp, 3 * SLOT, quarter)

    mixed = cell(
        first,
        gain_mix[None],
        w_query,
        w_key,
        w_value,
        w_outgate,
        w_input_gate.T,
        w_forget_gate.T,
        cell_state[:, 0],
        norm_state[:, 0],
        max_state,
    )[0]
    sent = to_all(jnp.concatenate([mixed, tokens], axis=1), near * tp)
    second = exchange(sent, NEAR + ("x",))
    second = second.reshape(near, tp, seqs, HEAD + quarter)
    group, outgoing, own_resid = residual(
        me, place, second, [mix_out[k] for k in range(tp)], gain_ffn[None], route_ids.T, experts
    )

    outgoing = outgoing.reshape(experts, 4, -1)
    received = exchange(outgoing, EP)

    rows = received.reshape(experts, -1)
    hidden = (jax.nn.silu(dot(rows, expert_gate[0])) * dot(rows, expert_up[0])).astype(bf16)
    partial = dot(hidden, expert_down[0]).astype(bf16).reshape(experts, 4, -1)
    returned = exchange(partial, EP)

    part = dense_branch(group, dense, mix_row)
    part = combine(place, part, returned.reshape(experts, -1), route_ids, route_weight, quarter)
    parts = exchange(part, NEAR + ("x",))
    total = own_resid.astype(f32) + parts.astype(f32).sum(axis=0)
    return total.astype(bf16)


def solution(mesh):
    fine = Mesh(mesh.devices.reshape(4, 2, 4, 2, 2, 4), EP + ("x",))
    return jax.shard_map(
        layer,
        mesh=fine,
        in_specs=(
            P(EP, "x"),
            P(),
            P(None, "x"),
            P(None, "x"),
            P(None, "x"),
            P(None, "x"),
            P(None, "x"),
            P(None, "x"),
            P(None, "x"),
            P(EP, "x", None, None),
            P(EP, "x", None),
            P(EP, "x"),
            P(),
            P(EP, None),
            P(EP, None),
            P(EP, None, "x"),
            P(EP, None, "x"),
            P(EP, "x", None),
            P("x", EP),
            P("x", EP),
            P(EP, "x"),
            P("x"),
        ),
        out_specs=P(EP, "x"),
        check_vma=False,
    )
```

```python
import jax
import jax.numpy as jnp
from jax import lax
from jax.experimental import pallas as pl
from jax.experimental.pallas import tpu as pltpu
from jax.sharding import Mesh, PartitionSpec as P

HEAD = 128

epsilon = 1e-06
f32 = jnp.float32
bf16 = jnp.bfloat16

FAR = ("zh", "yh", "c")
NEAR = ("zl", "yl")
SLOT = 8
EP = ("zh", "zl", "yh", "yl", "c")


def exchange(blocks, axis):
    return lax.all_to_all(blocks, axis, 0, 0, tiled=True)


def dot(a, b):
    return jnp.dot(a, b, preferred_element_type=f32)


def dot_turned(a, b):
    return lax.dot_general(a, b, (((1,), (1,)), ((), ())), preferred_element_type=f32)


def shifted(array, axis, step):
    size = lax.axis_size(axis)
    return lax.ppermute(array, axis, [(i, (i + step) % size) for i in range(size)])


def upright(row):
    count = row.shape[1]
    square = (count, count)
    same = lax.broadcasted_iota(jnp.int32, square, 0) == lax.broadcasted_iota(jnp.int32, square, 1)
    return jnp.sum(jnp.where(same, jnp.broadcast_to(row, square), 0.0), axis=1, keepdims=True)


def pack_kernel(tokens, gate, up, down, mix, out):
    seqs, quarter = tokens.shape
    count, columns = out.shape[0], gate.shape[0]
    slim = columns // count
    room = out.shape[1] - seqs
    source = jnp.concatenate([gate[...], up[...], down[...]], axis=0)
    row = lax.broadcasted_iota(jnp.int32, (room, 3 * columns), 0)
    column = lax.broadcasted_iota(jnp.int32, (room, 3 * columns), 1)
    slot = row & (SLOT - 1)
    wanted = slot + lax.div(row, SLOT) * columns
    last = lax.broadcasted_iota(jnp.int32, (room, quarter), 0) == 3 * SLOT
    extra = jnp.where(last, jnp.broadcast_to(mix[...].astype(f32)[None], (room, quarter)), 0.0)
    for k in range(count):
        pick = (column == wanted + k * slim) & (slot < slim) & (row < 3 * SLOT)
        out[k, :seqs] = tokens[...]
        out[k, seqs:] = (dot(pick.astype(f32).astype(bf16), source) + extra).astype(bf16)


def pack(tokens, gate, up, down, mix, count):
    seqs, quarter = tokens.shape
    return pl.pallas_call(
        pack_kernel,
        out_shape=jax.ShapeDtypeStruct((count, seqs + 4 * SLOT, quarter), bf16),
        name="pack",
    )(tokens, gate, up, down, mix)


def cell_kernel(first, gain, wq, wk, wv, wo, wi, wf, state, norm, peak, tokens, out):
    seqs = norm.shape[0]
    values = jnp.concatenate([first[k, :seqs] for k in range(first.shape[0])], axis=1).astype(f32)
    scale = lax.rsqrt(jnp.mean(values * values, axis=1, keepdims=True) + epsilon)
    rows = (values * scale * gain[...]).astype(bf16)
    query = dot(rows, wq[...])
    key = dot(rows, wk[...]) * HEAD ** (-0.5)
    value = dot(rows, wv[...])
    gate = jax.nn.sigmoid(dot(rows, wo[...]))
    wide = rows.astype(f32)
    enter = jnp.sum(wide * wi[...].astype(f32), axis=1, keepdims=True)
    forget = jnp.sum(wide * wf[...].astype(f32), axis=1, keepdims=True)
    carried = jnp.minimum(forget, 0.0) - jnp.log1p(jnp.exp(-jnp.abs(forget))) + upright(peak[...])
    stabilizer = jnp.maximum(carried, enter)
    old = jnp.exp(carried - stabilizer)
    new = jnp.exp(enter - stabilizer) * jnp.sum(query * key, axis=1, keepdims=True)
    turned = query.T
    read = [
        jnp.sum(turned[:, b : b + 1] * state[b], axis=0, keepdims=True) for b in range(seqs)
    ]
    numerator = old * jnp.concatenate(read, axis=0) + new * value
    denominator = old * jnp.sum(query * norm[...], axis=1, keepdims=True) + new
    mixed = gate * (numerator / jnp.maximum(jnp.abs(denominator), 1.0))
    mixed = mixed.astype(bf16)
    for k in range(out.shape[0]):
        out[k, :, :HEAD] = mixed
        out[k, :, HEAD:] = tokens[...]


def cell(first, gain, wq, wk, wv, wo, wi, wf, state, norm, peak, tokens, count):
    return pl.pallas_call(
        cell_kernel,
        out_shape=jax.ShapeDtypeStruct((count, norm.shape[0], HEAD + tokens.shape[1]), bf16),
        cost_estimate=pl.CostEstimate(flops=40000000, bytes_accessed=2200000, transcendentals=9000),
        name="cell",
    )(first, gain, wq, wk, wv, wo, wi, wf, state, norm, peak, tokens)


def residual_kernel(me, place, second, w0, w1, w2, w3, gain, ids, group, outgoing, own, resid):
    near, tp, seqs, _ = second.shape
    quarter = w0.shape[1]
    heads = jnp.concatenate(
        [
            jnp.concatenate([second[s, k, :, :HEAD] for s in range(near)], axis=0)
            for k in range(tp)
        ],
        axis=1,
    )
    total = jnp.zeros((near * seqs, 1), f32)
    for step, weight in enumerate((w0, w1, w2, w3)):
        k = (me[0] + tp - step) & (tp - 1)
        added = dot(heads, weight[...])
        old = jnp.concatenate([second[s, k, :, HEAD:] for s in range(near)], axis=0)
        values = (old.astype(f32) + added).astype(bf16)
        wide = values.astype(f32)
        total = total + jnp.sum(wide * wide, axis=1, keepdims=True)
        resid[:, pl.ds(pl.multiple_of(k * quarter, quarter), quarter)] = wide
        if step == 0:
            group[:, :quarter] = values
    start = pl.multiple_of(place[0] * seqs, seqs)
    own[...] = group[pl.ds(start, seqs), :quarter]
    scale = lax.rsqrt(total * (1.0 / (tp * quarter)) + epsilon)
    group[...] = (resid[...] * scale * gain[...]).astype(bf16)
    experts = outgoing.shape[0]
    expert = lax.broadcasted_iota(jnp.int32, (experts, seqs), 0)
    chosen = ((expert == ids[0:1, :]) | (expert == ids[1:2, :])).astype(f32).astype(bf16)
    rows = dot(chosen, group[pl.ds(start, seqs), :])
    for k in range(tp):
        outgoing[:, k, :] = rows[:, k * quarter : (k + 1) * quarter].astype(bf16)


def residual(me, place, second, weights, gain, ids, experts):
    near, tp, seqs, _ = second.shape
    quarter = weights[0].shape[1]
    whole = pl.BlockSpec(memory_space=pltpu.VMEM)
    scalar = pl.BlockSpec(memory_space=pltpu.SMEM)
    return pl.pallas_call(
        residual_kernel,
        out_shape=(
            jax.ShapeDtypeStruct((near * seqs, tp * quarter), bf16),
            jax.ShapeDtypeStruct((experts, tp, quarter), bf16),
            jax.ShapeDtypeStruct((seqs, quarter), bf16),
        ),
        in_specs=[scalar, scalar] + [whole] * 7,
        out_specs=(whole, whole, whole),
        scratch_shapes=[pltpu.VMEM((near * seqs, tp * quarter), f32)],
        cost_estimate=pl.CostEstimate(flops=140000000, bytes_accessed=2000000, transcendentals=128),
        compiler_params=pltpu.CompilerParams(vmem_limit_bytes=12 << 20),
        name="residual",
    )(me[None], place[None], second, *weights, gain, ids)


def dense_kernel(group, weights, mix, out):
    far, tp, _, quarter = weights.shape

    def matrix(k, place):
        return weights[:, k, place * SLOT : (place + 1) * SLOT].reshape(far * SLOT, quarter)

    rows = group[...]
    gate, up = 0.0, 0.0
    for k in range(tp):
        part = rows[:, k * quarter : (k + 1) * quarter]
        gate = gate + dot_turned(part, matrix(k, 0))
        up = up + dot_turned(part, matrix(k, 1))
    hidden = (gate * jax.nn.sigmoid(gate) * up).astype(bf16)
    logit = jnp.sum(rows.astype(f32) * mix[...].astype(f32), axis=1, keepdims=True)
    mix_gate = jax.nn.sigmoid(logit)
    for k in range(tp):
        out[:, k * quarter : (k + 1) * quarter] = mix_gate * dot(hidden, matrix(k, 2))


def dense_branch(group, weights, mix):
    return pl.pallas_call(
        dense_kernel,
        out_shape=jax.ShapeDtypeStruct(group.shape, f32),
        compiler_params=pltpu.CompilerParams(vmem_limit_bytes=12 << 20),
        cost_estimate=pl.CostEstimate(flops=100000000, bytes_accessed=1800000, transcendentals=32000),
        name="dense",
    )(group, weights, mix)


def expert_kernel(rows, gate, up, down, out):
    parts, width = rows.shape[1:]
    here = jnp.concatenate([rows[:, k, :] for k in range(parts)], axis=1)
    opened = dot_turned(here, gate[...])
    hidden = opened * jax.nn.sigmoid(opened) * dot_turned(here, up[...])
    result = dot(hidden.astype(bf16), down[...]).astype(bf16)
    for k in range(parts):
        out[:, k, :] = result[:, k * width : (k + 1) * width]


def expert(rows, gate, up, down):
    return pl.pallas_call(
        expert_kernel,
        out_shape=jax.ShapeDtypeStruct(rows.shape, bf16),
        compiler_params=pltpu.CompilerParams(vmem_limit_bytes=12 << 20),
        cost_estimate=pl.CostEstimate(flops=277000000, bytes_accessed=2700000, transcendentals=45000),
        name="expert",
    )(rows, gate, up, down)


def combine_kernel(place, part, returned, ids, weights, out):
    seqs, quarter = out.shape[1:]
    experts, tp, _ = returned.shape
    expert = lax.broadcasted_iota(jnp.int32, (seqs, experts), 1)
    here = ids[...]
    ahead, behind = upright(weights[0:1]), upright(weights[1:2])
    rows = jnp.concatenate([returned[:, k, :] for k in range(tp)], axis=1)
    first = dot((expert == here[:, 0:1]).astype(f32).astype(bf16), rows)
    second = dot((expert == here[:, 1:2]).astype(f32).astype(bf16), rows)
    moe = ahead * first + behind * second
    for s in range(out.shape[0] // tp):
        mine = jnp.where(place[0] == s, 1.0, 0.0)
        for k in range(tp):
            columns = slice(k * quarter, (k + 1) * quarter)
            value = part[s * seqs : (s + 1) * seqs, columns] + mine * moe[:, columns]
            out[s * tp + k] = value.astype(bf16)


def combine(place, part, returned, ids, weights, quarter):
    seqs = ids.shape[0]
    whole = pl.BlockSpec(memory_space=pltpu.VMEM)
    count = part.shape[0] // seqs * (part.shape[1] // quarter)
    return pl.pallas_call(
        combine_kernel,
        out_shape=jax.ShapeDtypeStruct((count, seqs, quarter), bf16),
        in_specs=[pl.BlockSpec(memory_space=pltpu.SMEM)] + [whole] * 4,
        out_specs=whole,
        compiler_params=pltpu.CompilerParams(vmem_limit_bytes=8 << 20),
        name="combine",
    )(place[None], part, returned, ids, weights)


def layer(
    tokens,
    gain_mix,
    w_query,
    w_key,
    w_value,
    w_outgate,
    w_input_gate,
    w_forget_gate,
    w_mix_out,
    cell_state,
    norm_state,
    max_state,
    gain_ffn,
    route_ids,
    route_logits,
    expert_gate,
    expert_up,
    expert_down,
    dense_gate,
    dense_up,
    dense_down,
    dense_mix,
):
    seqs, quarter = tokens.shape
    tp = lax.axis_size("x")
    far = lax.axis_size(FAR)
    near = lax.axis_size(NEAR)
    experts = lax.axis_size(EP)
    me = lax.axis_index("x")
    place = lax.axis_index(NEAR)

    sent = pack(tokens, dense_gate.T, dense_up.T, dense_down, dense_mix, tp)
    first = exchange(sent, "x")
    mix_row = first[:, seqs + 3 * SLOT].reshape(1, -1)

    turned_logits = route_logits.T
    route_weight = jax.nn.sigmoid(turned_logits - turned_logits[::-1])

    mix_out = {0: w_mix_out}
    for step in (2, 1, 3):
        mix_out[step] = shifted(w_mix_out, "x", step)

    dense = lax.all_gather(first[:, seqs : seqs + 3 * SLOT].reshape(-1, quarter), FAR)
    dense = dense.reshape(far, tp, 3 * SLOT, quarter)

    sent = cell(
        first,
        gain_mix[None],
        w_query,
        w_key,
        w_value,
        w_outgate,
        w_input_gate.T,
        w_forget_gate.T,
        cell_state[:, 0],
        norm_state[:, 0],
        max_state.T,
        tokens,
        near * tp,
    )
    second = exchange(sent, NEAR + ("x",))
    second = second.reshape(near, tp, seqs, HEAD + quarter)
    group, outgoing, own_resid = residual(
        me, place, second, [mix_out[k] for k in range(tp)], gain_ffn[None], route_ids.T, experts
    )

    received = exchange(outgoing, EP)

    partial = expert(received, expert_gate[0].T, expert_up[0].T, expert_down[0])
    returned = exchange(partial, EP)

    part = dense_branch(group, dense, mix_row)
    part = combine(place, part, returned, route_ids, route_weight, quarter)
    parts = exchange(part, NEAR + ("x",))
    total = own_resid.astype(f32) + parts.astype(f32).sum(axis=0)
    return total.astype(bf16)


def solution(mesh):
    fine = Mesh(mesh.devices.reshape(4, 2, 4, 2, 2, 4), EP + ("x",))
    return jax.shard_map(
        layer,
        mesh=fine,
        in_specs=(
            P(EP, "x"),
            P(),
            P(None, "x"),
            P(None, "x"),
            P(None, "x"),
            P(None, "x"),
            P(None, "x"),
            P(None, "x"),
            P(None, "x"),
            P(EP, "x", None, None),
            P(EP, "x", None),
            P(EP, "x"),
            P(),
            P(EP, None),
            P(EP, None),
            P(EP, None, "x"),
            P(EP, None, "x"),
            P(EP, "x", None),
            P("x", EP),
            P("x", EP),
            P(EP, "x"),
            P("x"),
        ),
        out_specs=P(EP, "x"),
        check_vma=False,
    )
```

```python
import jax
import jax.numpy as jnp
from jax import lax
from jax.experimental import pallas as pl
from jax.experimental.pallas import tpu as pltpu
from jax.sharding import Mesh, PartitionSpec as P

HEAD = 128

epsilon = 1e-06
f32 = jnp.float32
bf16 = jnp.bfloat16

FAR = ("zh", "yh", "c")
NEAR = ("zl", "yl")
SLOT = 8
EP = ("zh", "zl", "yh", "yl", "c")


def exchange(blocks, axis):
    return lax.all_to_all(blocks, axis, 0, 0, tiled=True)


def dot(a, b):
    return jnp.dot(a, b, preferred_element_type=f32)


def dot_turned(a, b):
    return lax.dot_general(a, b, (((1,), (1,)), ((), ())), preferred_element_type=f32)


def shifted(array, axis, step):
    size = lax.axis_size(axis)
    return lax.ppermute(array, axis, [(i, (i + step) % size) for i in range(size)])


def upright(row):
    count = row.shape[1]
    square = (count, count)
    same = lax.broadcasted_iota(jnp.int32, square, 0) == lax.broadcasted_iota(jnp.int32, square, 1)
    return jnp.sum(jnp.where(same, jnp.broadcast_to(row, square), 0.0), axis=1, keepdims=True)


def pack_kernel(tokens, gate, up, down, mix, out):
    seqs, quarter = tokens.shape
    count, columns = out.shape[0], gate.shape[0]
    slim = columns // count
    room = out.shape[1] - seqs
    source = jnp.concatenate([gate[...], up[...], down[...]], axis=0)
    row = lax.broadcasted_iota(jnp.int32, (room, 3 * columns), 0)
    column = lax.broadcasted_iota(jnp.int32, (room, 3 * columns), 1)
    slot = row & (SLOT - 1)
    wanted = slot + lax.div(row, SLOT) * columns
    last = lax.broadcasted_iota(jnp.int32, (room, quarter), 0) == 3 * SLOT
    extra = jnp.where(last, jnp.broadcast_to(mix[...].astype(f32)[None], (room, quarter)), 0.0)
    for k in range(count):
        pick = (column == wanted + k * slim) & (slot < slim) & (row < 3 * SLOT)
        out[k, :seqs] = tokens[...]
        out[k, seqs:] = (dot(pick.astype(f32).astype(bf16), source) + extra).astype(bf16)


def pack(tokens, gate, up, down, mix, count):
    seqs, quarter = tokens.shape
    return pl.pallas_call(
        pack_kernel,
        out_shape=jax.ShapeDtypeStruct((count, seqs + 4 * SLOT, quarter), bf16),
        name="pack",
    )(tokens, gate, up, down, mix)


def cell_kernel(*refs):
    count = (len(refs) - 2) // 2
    stored, out, kept, arrived = refs[:count], refs[count], refs[count + 1 : -1], refs[-1]
    copies = [
        pltpu.make_async_copy(stored[k], kept[k], arrived.at[k]) for k in range(count)
    ]
    for copy in copies:
        copy.start()
    for copy in copies[:-1]:
        copy.wait()
    first, gain, wq, wk, wv, wo, wi, wf, norm, peak, tokens, state = kept
    seqs = norm.shape[0]
    values = jnp.concatenate([first[k, :seqs] for k in range(first.shape[0])], axis=1).astype(f32)
    scale = lax.rsqrt(jnp.mean(values * values, axis=1, keepdims=True) + epsilon)
    rows = (values * scale * gain[...]).astype(bf16)
    query = dot(rows, wq[...])
    key = dot(rows, wk[...]) * HEAD ** (-0.5)
    value = dot(rows, wv[...])
    gate = jax.nn.sigmoid(dot(rows, wo[...]))
    wide = rows.astype(f32)
    enter = jnp.sum(wide * wi[...].astype(f32), axis=1, keepdims=True)
    forget = jnp.sum(wide * wf[...].astype(f32), axis=1, keepdims=True)
    carried = jnp.minimum(forget, 0.0) - jnp.log1p(jnp.exp(-jnp.abs(forget))) + upright(peak[...])
    stabilizer = jnp.maximum(carried, enter)
    old = jnp.exp(carried - stabilizer)
    new = jnp.exp(enter - stabilizer) * jnp.sum(query * key, axis=1, keepdims=True)
    turned = query.T
    copies[-1].wait()
    read = [
        jnp.sum(turned[:, b : b + 1] * state[b], axis=0, keepdims=True) for b in range(seqs)
    ]
    numerator = old * jnp.concatenate(read, axis=0) + new * value
    denominator = old * jnp.sum(query * norm[...], axis=1, keepdims=True) + new
    mixed = gate * (numerator / jnp.maximum(jnp.abs(denominator), 1.0))
    mixed = mixed.astype(bf16)
    for k in range(out.shape[0]):
        out[k, :, :HEAD] = mixed
        out[k, :, HEAD:] = tokens[...]


def cell(first, gain, wq, wk, wv, wo, wi, wf, state, norm, peak, tokens, count):
    stored = (first, gain, wq, wk, wv, wo, wi, wf, norm, peak, tokens, state)
    away = pl.BlockSpec(memory_space=pltpu.HBM)
    here = pl.BlockSpec(memory_space=pltpu.VMEM)
    return pl.pallas_call(
        cell_kernel,
        out_shape=jax.ShapeDtypeStruct((count, norm.shape[0], HEAD + tokens.shape[1]), bf16),
        in_specs=[away] * len(stored),
        out_specs=here,
        scratch_shapes=[pltpu.VMEM(a.shape, a.dtype) for a in stored]
        + [pltpu.SemaphoreType.DMA((len(stored),))],
        cost_estimate=pl.CostEstimate(flops=40000000, bytes_accessed=2200000, transcendentals=9000),
        name="cell",
    )(*stored)


def residual_kernel(me, place, second, w0, w1, w2, w3, gain, ids, group, outgoing, own, resid):
    near, tp, seqs, _ = second.shape
    quarter = w0.shape[1]
    heads = jnp.concatenate(
        [
            jnp.concatenate([second[s, k, :, :HEAD] for s in range(near)], axis=0)
            for k in range(tp)
        ],
        axis=1,
    )
    total = jnp.zeros((near * seqs, 1), f32)
    for step, weight in enumerate((w0, w1, w2, w3)):
        k = (me[0] + tp - step) & (tp - 1)
        added = dot(heads, weight[...])
        old = jnp.concatenate([second[s, k, :, HEAD:] for s in range(near)], axis=0)
        values = (old.astype(f32) + added).astype(bf16)
        wide = values.astype(f32)
        total = total + jnp.sum(wide * wide, axis=1, keepdims=True)
        resid[:, pl.ds(pl.multiple_of(k * quarter, quarter), quarter)] = wide
        if step == 0:
            group[:, :quarter] = values
    start = pl.multiple_of(place[0] * seqs, seqs)
    own[...] = group[pl.ds(start, seqs), :quarter]
    scale = lax.rsqrt(total * (1.0 / (tp * quarter)) + epsilon)
    group[...] = (resid[...] * scale * gain[...]).astype(bf16)
    experts = outgoing.shape[0]
    expert = lax.broadcasted_iota(jnp.int32, (experts, seqs), 0)
    chosen = ((expert == ids[0:1, :]) | (expert == ids[1:2, :])).astype(f32).astype(bf16)
    rows = dot(chosen, group[pl.ds(start, seqs), :])
    for k in range(tp):
        outgoing[:, k, :] = rows[:, k * quarter : (k + 1) * quarter].astype(bf16)


def residual(me, place, second, weights, gain, ids, experts):
    near, tp, seqs, _ = second.shape
    quarter = weights[0].shape[1]
    whole = pl.BlockSpec(memory_space=pltpu.VMEM)
    scalar = pl.BlockSpec(memory_space=pltpu.SMEM)
    return pl.pallas_call(
        residual_kernel,
        out_shape=(
            jax.ShapeDtypeStruct((near * seqs, tp * quarter), bf16),
            jax.ShapeDtypeStruct((experts, tp, quarter), bf16),
            jax.ShapeDtypeStruct((seqs, quarter), bf16),
        ),
        in_specs=[scalar, scalar] + [whole] * 7,
        out_specs=(whole, whole, whole),
        scratch_shapes=[pltpu.VMEM((near * seqs, tp * quarter), f32)],
        cost_estimate=pl.CostEstimate(flops=140000000, bytes_accessed=2000000, transcendentals=128),
        compiler_params=pltpu.CompilerParams(vmem_limit_bytes=12 << 20),
        name="residual",
    )(me[None], place[None], second, *weights, gain, ids)


def dense_kernel(group, weights, mix, out):
    far, tp, _, quarter = weights.shape

    def matrix(k, place):
        return weights[:, k, place * SLOT : (place + 1) * SLOT].reshape(far * SLOT, quarter)

    rows = group[...]
    gate, up = 0.0, 0.0
    for k in range(tp):
        part = rows[:, k * quarter : (k + 1) * quarter]
        gate = gate + dot_turned(part, matrix(k, 0))
        up = up + dot_turned(part, matrix(k, 1))
    hidden = (gate * jax.nn.sigmoid(gate) * up).astype(bf16)
    logit = jnp.sum(rows.astype(f32) * mix[...].astype(f32), axis=1, keepdims=True)
    mix_gate = jax.nn.sigmoid(logit)
    for k in range(tp):
        out[:, k * quarter : (k + 1) * quarter] = mix_gate * dot(hidden, matrix(k, 2))


def dense_branch(group, weights, mix):
    return pl.pallas_call(
        dense_kernel,
        out_shape=jax.ShapeDtypeStruct(group.shape, f32),
        compiler_params=pltpu.CompilerParams(vmem_limit_bytes=12 << 20),
        cost_estimate=pl.CostEstimate(flops=100000000, bytes_accessed=1800000, transcendentals=32000),
        name="dense",
    )(group, weights, mix)


def expert_kernel(rows, gate, up, down, out):
    parts, width = rows.shape[1:]
    here = jnp.concatenate([rows[:, k, :] for k in range(parts)], axis=1)
    opened = dot_turned(here, gate[...])
    hidden = opened * jax.nn.sigmoid(opened) * dot_turned(here, up[...])
    result = dot(hidden.astype(bf16), down[...]).astype(bf16)
    for k in range(parts):
        out[:, k, :] = result[:, k * width : (k + 1) * width]


def expert(rows, gate, up, down):
    return pl.pallas_call(
        expert_kernel,
        out_shape=jax.ShapeDtypeStruct(rows.shape, bf16),
        compiler_params=pltpu.CompilerParams(vmem_limit_bytes=12 << 20),
        cost_estimate=pl.CostEstimate(flops=277000000, bytes_accessed=2700000, transcendentals=45000),
        name="expert",
    )(rows, gate, up, down)


def combine_kernel(mine, part, returned, ids, weights, out):
    seqs, quarter = out.shape[1:]
    experts, tp, _ = returned.shape
    expert = lax.broadcasted_iota(jnp.int32, (seqs, experts), 1)
    here = ids[...]
    ahead, behind = upright(weights[0:1]), upright(weights[1:2])
    rows = jnp.concatenate([returned[:, k, :] for k in range(tp)], axis=1)
    first = dot((expert == here[:, 0:1]).astype(f32).astype(bf16), rows)
    second = dot((expert == here[:, 1:2]).astype(f32).astype(bf16), rows)
    moe = ahead * first + behind * second
    for s in range(out.shape[0] // tp):
        for k in range(tp):
            columns = slice(k * quarter, (k + 1) * quarter)
            value = part[s * seqs : (s + 1) * seqs, columns] + mine[s] * moe[:, columns]
            out[s * tp + k] = value.astype(bf16)


def combine(mine, part, returned, ids, weights, quarter):
    seqs = ids.shape[0]
    whole = pl.BlockSpec(memory_space=pltpu.VMEM)
    count = part.shape[0] // seqs * (part.shape[1] // quarter)
    return pl.pallas_call(
        combine_kernel,
        out_shape=jax.ShapeDtypeStruct((count, seqs, quarter), bf16),
        in_specs=[pl.BlockSpec(memory_space=pltpu.SMEM)] + [whole] * 4,
        out_specs=whole,
        compiler_params=pltpu.CompilerParams(vmem_limit_bytes=8 << 20),
        name="combine",
    )(mine, part, returned, ids, weights)


def layer(
    tokens,
    gain_mix,
    w_query,
    w_key,
    w_value,
    w_outgate,
    w_input_gate,
    w_forget_gate,
    w_mix_out,
    cell_state,
    norm_state,
    max_state,
    gain_ffn,
    route_ids,
    route_logits,
    expert_gate,
    expert_up,
    expert_down,
    dense_gate,
    dense_up,
    dense_down,
    dense_mix,
):
    seqs, quarter = tokens.shape
    tp = lax.axis_size("x")
    far = lax.axis_size(FAR)
    near = lax.axis_size(NEAR)
    experts = lax.axis_size(EP)
    me = lax.axis_index("x")
    place = lax.axis_index(NEAR)

    sent = pack(tokens, dense_gate.T, dense_up.T, dense_down, dense_mix, tp)
    first = exchange(sent, "x")
    mix_row = first[:, seqs + 3 * SLOT].reshape(1, -1)

    turned_logits = route_logits.T
    route_weight = jax.nn.sigmoid(turned_logits - turned_logits[::-1])
    mine = (jnp.arange(near, dtype=jnp.int32) == place).astype(f32)

    mix_out = {0: w_mix_out}
    for step in (2, 1, 3):
        mix_out[step] = shifted(w_mix_out, "x", step)

    dense = lax.all_gather(first[:, seqs : seqs + 3 * SLOT].reshape(-1, quarter), FAR)
    dense = dense.reshape(far, tp, 3 * SLOT, quarter)

    sent = cell(
        first,
        gain_mix[None],
        w_query,
        w_key,
        w_value,
        w_outgate,
        w_input_gate.T,
        w_forget_gate.T,
        cell_state[:, 0],
        norm_state[:, 0],
        max_state.T,
        tokens,
        near * tp,
    )
    second = exchange(sent, NEAR + ("x",))
    second = second.reshape(near, tp, seqs, HEAD + quarter)
    group, outgoing, own_resid = residual(
        me, place, second, [mix_out[k] for k in range(tp)], gain_ffn[None], route_ids.T, experts
    )

    received = exchange(outgoing, EP)

    partial = expert(received, expert_gate[0].T, expert_up[0].T, expert_down[0])
    returned = exchange(partial, EP)

    part = dense_branch(group, dense, mix_row)
    part = combine(mine, part, returned, route_ids, route_weight, quarter)
    parts = exchange(part, NEAR + ("x",))
    total = own_resid.astype(f32) + parts.astype(f32).sum(axis=0)
    return total.astype(bf16)


def solution(mesh):
    fine = Mesh(mesh.devices.reshape(4, 2, 4, 2, 2, 4), EP + ("x",))
    return jax.shard_map(
        layer,
        mesh=fine,
        in_specs=(
            P(EP, "x"),
            P(),
            P(None, "x"),
            P(None, "x"),
            P(None, "x"),
            P(None, "x"),
            P(None, "x"),
            P(None, "x"),
            P(None, "x"),
            P(EP, "x", None, None),
            P(EP, "x", None),
            P(EP, "x"),
            P(),
            P(EP, None),
            P(EP, None),
            P(EP, None, "x"),
            P(EP, None, "x"),
            P(EP, "x", None),
            P("x", EP),
            P("x", EP),
            P(EP, "x"),
            P("x"),
        ),
        out_specs=P(EP, "x"),
        check_vma=False,
    )
```

```python
import jax
import jax.numpy as jnp
from jax import lax
from jax.experimental import pallas as pl
from jax.experimental.pallas import tpu as pltpu
from jax.sharding import Mesh, PartitionSpec as P

HEAD = 128

epsilon = 1e-06
f32 = jnp.float32
bf16 = jnp.bfloat16

FAR = ("zh", "yh", "c")
NEAR = ("zl", "yl")
SLOT = 8
EP = ("zh", "zl", "yh", "yl", "c")


def exchange(blocks, axis):
    return lax.all_to_all(blocks, axis, 0, 0, tiled=True)


def dot(a, b):
    return jnp.dot(a, b, preferred_element_type=f32)


def dot_turned(a, b):
    return lax.dot_general(a, b, (((1,), (1,)), ((), ())), preferred_element_type=f32)


def shifted(array, axis, step):
    size = lax.axis_size(axis)
    return lax.ppermute(array, axis, [(i, (i + step) % size) for i in range(size)])


def upright(row):
    count = row.shape[1]
    square = (count, count)
    same = lax.broadcasted_iota(jnp.int32, square, 0) == lax.broadcasted_iota(jnp.int32, square, 1)
    return jnp.sum(jnp.where(same, jnp.broadcast_to(row, square), 0.0), axis=1, keepdims=True)


def pack_kernel(tokens, gate, up, down, mix, out):
    seqs, quarter = tokens.shape
    count, columns = out.shape[0], gate.shape[0]
    slim = columns // count
    room = out.shape[1] - seqs
    source = jnp.concatenate([gate[...], up[...], down[...]], axis=0)
    row = lax.broadcasted_iota(jnp.int32, (room, 3 * columns), 0)
    column = lax.broadcasted_iota(jnp.int32, (room, 3 * columns), 1)
    slot = row & (SLOT - 1)
    wanted = slot + lax.div(row, SLOT) * columns
    last = lax.broadcasted_iota(jnp.int32, (room, quarter), 0) == 3 * SLOT
    extra = jnp.where(last, jnp.broadcast_to(mix[...].astype(f32)[None], (room, quarter)), 0.0)
    for k in range(count):
        pick = (column == wanted + k * slim) & (slot < slim) & (row < 3 * SLOT)
        out[k, :seqs] = tokens[...]
        out[k, seqs:] = (dot(pick.astype(f32).astype(bf16), source) + extra).astype(bf16)


def pack(tokens, gate, up, down, mix, count):
    seqs, quarter = tokens.shape
    return pl.pallas_call(
        pack_kernel,
        out_shape=jax.ShapeDtypeStruct((count, seqs + 4 * SLOT, quarter), bf16),
        name="pack",
    )(tokens, gate, up, down, mix)


def cell_kernel(*refs):
    count = (len(refs) - 2) // 2
    stored, out, kept, arrived = refs[:count], refs[count], refs[count + 1 : -1], refs[-1]
    copies = [
        pltpu.make_async_copy(stored[k], kept[k], arrived.at[k]) for k in range(count)
    ]
    for copy in copies:
        copy.start()
    for copy in copies[:-1]:
        copy.wait()
    first, gain, wq, wk, wv, wo, wi, wf, norm, peak, state = kept
    seqs = norm.shape[0]
    values = jnp.concatenate([first[k, :seqs] for k in range(first.shape[0])], axis=1).astype(f32)
    scale = lax.rsqrt(jnp.mean(values * values, axis=1, keepdims=True) + epsilon)
    rows = (values * scale * gain[...]).astype(bf16)
    query = dot(rows, wq[...])
    key = dot(rows, wk[...]) * HEAD ** (-0.5)
    value = dot(rows, wv[...])
    gate = jax.nn.sigmoid(dot(rows, wo[...]))
    wide = rows.astype(f32)
    enter = jnp.sum(wide * wi[...].astype(f32), axis=1, keepdims=True)
    forget = jnp.sum(wide * wf[...].astype(f32), axis=1, keepdims=True)
    carried = jnp.minimum(forget, 0.0) - jnp.log1p(jnp.exp(-jnp.abs(forget))) + upright(peak[...])
    stabilizer = jnp.maximum(carried, enter)
    old = jnp.exp(carried - stabilizer)
    new = jnp.exp(enter - stabilizer) * jnp.sum(query * key, axis=1, keepdims=True)
    turned = query.T
    copies[-1].wait()
    read = [
        jnp.sum(turned[:, b : b + 1] * state[b], axis=0, keepdims=True) for b in range(seqs)
    ]
    numerator = old * jnp.concatenate(read, axis=0) + new * value
    denominator = old * jnp.sum(query * norm[...], axis=1, keepdims=True) + new
    mixed = gate * (numerator / jnp.maximum(jnp.abs(denominator), 1.0))
    mixed = mixed.astype(bf16)
    for k in range(out.shape[0]):
        out[k] = mixed


def cell(first, gain, wq, wk, wv, wo, wi, wf, state, norm, peak, count):
    stored = (first, gain, wq, wk, wv, wo, wi, wf, norm, peak, state)
    away = pl.BlockSpec(memory_space=pltpu.HBM)
    here = pl.BlockSpec(memory_space=pltpu.VMEM)
    return pl.pallas_call(
        cell_kernel,
        out_shape=jax.ShapeDtypeStruct((count, *norm.shape), bf16),
        in_specs=[away] * len(stored),
        out_specs=here,
        scratch_shapes=[pltpu.VMEM(a.shape, a.dtype) for a in stored]
        + [pltpu.SemaphoreType.DMA((len(stored),))],
        cost_estimate=pl.CostEstimate(flops=40000000, bytes_accessed=2200000, transcendentals=9000),
        name="cell",
    )(*stored)


def residual_kernel(me, second, first, w0, w1, w2, w3, gain, ids, normed, outgoing, own, resid):
    tp, seqs, _ = second.shape
    quarter = w0.shape[1]
    heads = jnp.concatenate([second[k] for k in range(tp)], axis=1)
    total = jnp.zeros((seqs, 1), f32)
    for step, weight in enumerate((w0, w1, w2, w3)):
        k = (me[0] + tp - step) & (tp - 1)
        values = (first[k, :seqs].astype(f32) + dot(heads, weight[...])).astype(bf16)
        wide = values.astype(f32)
        total = total + jnp.sum(wide * wide, axis=1, keepdims=True)
        resid[:, pl.ds(pl.multiple_of(k * quarter, quarter), quarter)] = wide
        if step == 0:
            own[...] = values
    scale = lax.rsqrt(total * (1.0 / (tp * quarter)) + epsilon)
    rows = (resid[...] * scale * gain[...]).astype(bf16)
    normed[...] = rows
    expert = lax.broadcasted_iota(jnp.int32, (outgoing.shape[0], seqs), 0)
    chosen = ((expert == ids[0:1, :]) | (expert == ids[1:2, :])).astype(f32).astype(bf16)
    sent = dot(chosen, rows)
    for k in range(tp):
        outgoing[:, k, :] = sent[:, k * quarter : (k + 1) * quarter].astype(bf16)


def residual(me, second, first, weights, gain, ids, experts):
    tp, seqs, _ = second.shape
    quarter = weights[0].shape[1]
    whole = pl.BlockSpec(memory_space=pltpu.VMEM)
    return pl.pallas_call(
        residual_kernel,
        out_shape=(
            jax.ShapeDtypeStruct((seqs, tp * quarter), bf16),
            jax.ShapeDtypeStruct((experts, tp, quarter), bf16),
            jax.ShapeDtypeStruct((seqs, quarter), bf16),
        ),
        in_specs=[pl.BlockSpec(memory_space=pltpu.SMEM)] + [whole] * 8,
        out_specs=(whole, whole, whole),
        scratch_shapes=[pltpu.VMEM((seqs, tp * quarter), f32)],
        compiler_params=pltpu.CompilerParams(vmem_limit_bytes=12 << 20),
        cost_estimate=pl.CostEstimate(flops=21000000, bytes_accessed=1500000, transcendentals=16),
        name="residual",
    )(me[None], second, first, *weights, gain, ids)


def dense_kernel(group, weights, mix, out):
    far, tp, _, quarter = weights.shape

    def matrix(k, place):
        return weights[:, k, place * SLOT : (place + 1) * SLOT].reshape(far * SLOT, quarter)

    rows = group[...]
    gate, up = 0.0, 0.0
    for k in range(tp):
        part = rows[:, k * quarter : (k + 1) * quarter]
        gate = gate + dot_turned(part, matrix(k, 0))
        up = up + dot_turned(part, matrix(k, 1))
    hidden = (gate * jax.nn.sigmoid(gate) * up).astype(bf16)
    logit = jnp.sum(rows.astype(f32) * mix[...].astype(f32), axis=1, keepdims=True)
    mix_gate = jax.nn.sigmoid(logit)
    for k in range(tp):
        out[:, k * quarter : (k + 1) * quarter] = mix_gate * dot(hidden, matrix(k, 2))


def dense_branch(group, weights, mix):
    return pl.pallas_call(
        dense_kernel,
        out_shape=jax.ShapeDtypeStruct(group.shape, f32),
        compiler_params=pltpu.CompilerParams(vmem_limit_bytes=12 << 20),
        cost_estimate=pl.CostEstimate(flops=100000000, bytes_accessed=1800000, transcendentals=32000),
        name="dense",
    )(group, weights, mix)


def expert_kernel(rows, gate, up, down, out):
    parts, width = rows.shape[1:]
    here = jnp.concatenate([rows[:, k, :] for k in range(parts)], axis=1)
    opened = dot_turned(here, gate[...])
    hidden = opened * jax.nn.sigmoid(opened) * dot_turned(here, up[...])
    result = dot(hidden.astype(bf16), down[...]).astype(bf16)
    for k in range(parts):
        out[:, k, :] = result[:, k * width : (k + 1) * width]


def expert(rows, gate, up, down):
    return pl.pallas_call(
        expert_kernel,
        out_shape=jax.ShapeDtypeStruct(rows.shape, bf16),
        compiler_params=pltpu.CompilerParams(vmem_limit_bytes=12 << 20),
        cost_estimate=pl.CostEstimate(flops=277000000, bytes_accessed=2700000, transcendentals=45000),
        name="expert",
    )(rows, gate, up, down)


def combine_kernel(slots, part, returned, ids, weights, out):
    seqs, quarter = out.shape[1:]
    experts, tp, _ = returned.shape
    expert = lax.broadcasted_iota(jnp.int32, (seqs, experts), 1)
    here = ids[...]
    ahead, behind = upright(weights[0:1]), upright(weights[1:2])
    rows = jnp.concatenate([returned[:, k, :] for k in range(tp)], axis=1)
    first = dot((expert == here[:, 0:1]).astype(f32).astype(bf16), rows)
    second = dot((expert == here[:, 1:2]).astype(f32).astype(bf16), rows)
    moe = ahead * first + behind * second
    for s in range(out.shape[0] // tp):
        for k in range(tp):
            columns = slice(k * quarter, (k + 1) * quarter)
            value = part[s * seqs : (s + 1) * seqs, columns]
            if s == 0:
                value = value + moe[:, columns]
            out[slots[s] + k] = value.astype(bf16)


def combine(slots, part, returned, ids, weights, quarter):
    seqs = ids.shape[0]
    whole = pl.BlockSpec(memory_space=pltpu.VMEM)
    count = part.shape[0] // seqs * (part.shape[1] // quarter)
    return pl.pallas_call(
        combine_kernel,
        out_shape=jax.ShapeDtypeStruct((count, seqs, quarter), bf16),
        in_specs=[pl.BlockSpec(memory_space=pltpu.SMEM)] + [whole] * 4,
        out_specs=whole,
        compiler_params=pltpu.CompilerParams(vmem_limit_bytes=8 << 20),
        name="combine",
    )(slots, part, returned, ids, weights)


def layer(
    tokens,
    gain_mix,
    w_query,
    w_key,
    w_value,
    w_outgate,
    w_input_gate,
    w_forget_gate,
    w_mix_out,
    cell_state,
    norm_state,
    max_state,
    gain_ffn,
    route_ids,
    route_logits,
    expert_gate,
    expert_up,
    expert_down,
    dense_gate,
    dense_up,
    dense_down,
    dense_mix,
):
    seqs, quarter = tokens.shape
    tp = lax.axis_size("x")
    far = lax.axis_size(FAR)
    near = lax.axis_size(NEAR)
    experts = lax.axis_size(EP)
    me = lax.axis_index("x")
    place = lax.axis_index(NEAR)

    sent = pack(tokens, dense_gate.T, dense_up.T, dense_down, dense_mix, tp)
    first = exchange(sent, "x")
    mix_row = first[:, seqs + 3 * SLOT].reshape(1, -1)

    turned_logits = route_logits.T
    route_weight = jax.nn.sigmoid(turned_logits - turned_logits[::-1])
    slots = (jnp.arange(near, dtype=jnp.int32) ^ place) * tp

    mix_out = {0: w_mix_out}
    for step in (2, 1, 3):
        mix_out[step] = shifted(w_mix_out, "x", step)

    dense = lax.all_gather(first[:, seqs : seqs + 3 * SLOT].reshape(-1, quarter), FAR)
    dense = dense.reshape(far, tp, 3 * SLOT, quarter)

    sent = cell(
        first,
        gain_mix[None],
        w_query,
        w_key,
        w_value,
        w_outgate,
        w_input_gate.T,
        w_forget_gate.T,
        cell_state[:, 0],
        norm_state[:, 0],
        max_state.T,
        tp,
    )
    second = exchange(sent, "x")
    group, outgoing, own_resid = residual(
        me, second, first, [mix_out[k] for k in range(tp)], gain_ffn[None], route_ids.T, experts
    )

    received = exchange(outgoing, EP)

    for axis in ("yl", "zl"):
        other = lax.ppermute(group, axis, [(0, 1), (1, 0)])
        group = jnp.concatenate([group, other], axis=0)

    partial = expert(received, expert_gate[0].T, expert_up[0].T, expert_down[0])
    returned = exchange(partial, EP)

    part = dense_branch(group, dense, mix_row)
    part = combine(slots, part, returned, route_ids, route_weight, quarter)
    parts = exchange(part, NEAR + ("x",))
    total = own_resid.astype(f32) + parts.astype(f32).sum(axis=0)
    return total.astype(bf16)


def solution(mesh):
    fine = Mesh(mesh.devices.reshape(4, 2, 4, 2, 2, 4), EP + ("x",))
    return jax.shard_map(
        layer,
        mesh=fine,
        in_specs=(
            P(EP, "x"),
            P(),
            P(None, "x"),
            P(None, "x"),
            P(None, "x"),
            P(None, "x"),
            P(None, "x"),
            P(None, "x"),
            P(None, "x"),
            P(EP, "x", None, None),
            P(EP, "x", None),
            P(EP, "x"),
            P(),
            P(EP, None),
            P(EP, None),
            P(EP, None, "x"),
            P(EP, None, "x"),
            P(EP, "x", None),
            P("x", EP),
            P("x", EP),
            P(EP, "x"),
            P("x"),
        ),
        out_specs=P(EP, "x"),
        check_vma=False,
    )
```

```python
import jax
import jax.numpy as jnp
from jax import lax
from jax.experimental import pallas as pl
from jax.experimental.pallas import tpu as pltpu
from jax.sharding import Mesh, PartitionSpec as P

HEAD = 128

epsilon = 1e-06
f32 = jnp.float32
bf16 = jnp.bfloat16

FAR = ("zh", "yh", "c")
NEAR = ("zl", "yl")
SLOT = 8
EP = ("zh", "zl", "yh", "yl", "c")


def exchange(blocks, axis):
    return lax.all_to_all(blocks, axis, 0, 0, tiled=True)


def dot(a, b):
    return jnp.dot(a, b, preferred_element_type=f32)


def dot_turned(a, b):
    return lax.dot_general(a, b, (((1,), (1,)), ((), ())), preferred_element_type=f32)


def shifted(array, axis, step):
    size = lax.axis_size(axis)
    return lax.ppermute(array, axis, [(i, (i + step) % size) for i in range(size)])


def upright(row):
    count = row.shape[1]
    square = (count, count)
    same = lax.broadcasted_iota(jnp.int32, square, 0) == lax.broadcasted_iota(jnp.int32, square, 1)
    return jnp.sum(jnp.where(same, jnp.broadcast_to(row, square), 0.0), axis=1, keepdims=True)


def pack_kernel(tokens, gate, up, down, mix, out):
    seqs, quarter = tokens.shape
    count, columns = out.shape[0], gate.shape[0]
    slim = columns // count
    room = out.shape[1] - seqs
    source = jnp.concatenate([gate[...], up[...], down[...]], axis=0)
    row = lax.broadcasted_iota(jnp.int32, (room, 3 * columns), 0)
    column = lax.broadcasted_iota(jnp.int32, (room, 3 * columns), 1)
    slot = row & (SLOT - 1)
    wanted = slot + lax.div(row, SLOT) * columns
    last = lax.broadcasted_iota(jnp.int32, (room, quarter), 0) == 3 * SLOT
    extra = jnp.where(last, jnp.broadcast_to(mix[...].astype(f32)[None], (room, quarter)), 0.0)
    for k in range(count):
        pick = (column == wanted + k * slim) & (slot < slim) & (row < 3 * SLOT)
        out[k, :seqs] = tokens[...]
        out[k, seqs:] = (dot(pick.astype(f32).astype(bf16), source) + extra).astype(bf16)


def pack(tokens, gate, up, down, mix, count):
    seqs, quarter = tokens.shape
    return pl.pallas_call(
        pack_kernel,
        out_shape=jax.ShapeDtypeStruct((count, seqs + 4 * SLOT, quarter), bf16),
        name="pack",
    )(tokens, gate, up, down, mix)


def cell_kernel(first, gain, wq, wk, wv, wo, wi, wf, norm, peak, tokens, state, out):
    seqs = norm.shape[0]
    values = jnp.concatenate([first[k, :seqs] for k in range(first.shape[0])], axis=1).astype(f32)
    scale = lax.rsqrt(jnp.mean(values * values, axis=1, keepdims=True) + epsilon)
    rows = (values * scale * gain[...]).astype(bf16)
    query = dot(rows, wq[...])
    key = dot(rows, wk[...]) * HEAD ** (-0.5)
    value = dot(rows, wv[...])
    gate = jax.nn.sigmoid(dot(rows, wo[...]))
    wide = rows.astype(f32)
    enter = jnp.sum(wide * wi[...].astype(f32), axis=1, keepdims=True)
    forget = jnp.sum(wide * wf[...].astype(f32), axis=1, keepdims=True)
    carried = jnp.minimum(forget, 0.0) - jnp.log1p(jnp.exp(-jnp.abs(forget))) + upright(peak[...])
    stabilizer = jnp.maximum(carried, enter)
    old = jnp.exp(carried - stabilizer)
    new = jnp.exp(enter - stabilizer) * jnp.sum(query * key, axis=1, keepdims=True)
    turned = query.T
    read = [
        jnp.sum(turned[:, b : b + 1] * state[b], axis=0, keepdims=True) for b in range(seqs)
    ]
    numerator = old * jnp.concatenate(read, axis=0) + new * value
    denominator = old * jnp.sum(query * norm[...], axis=1, keepdims=True) + new
    mixed = gate * (numerator / jnp.maximum(jnp.abs(denominator), 1.0))
    mixed = mixed.astype(bf16)
    for k in range(out.shape[0]):
        out[k, :, :HEAD] = mixed
        out[k, :, HEAD:] = tokens[...]


def cell(first, gain, wq, wk, wv, wo, wi, wf, state, norm, peak, tokens, count):
    stored = (first, gain, wq, wk, wv, wo, wi, wf, norm, peak, tokens, state)
    return pl.pallas_call(
        cell_kernel,
        out_shape=jax.ShapeDtypeStruct((count, norm.shape[0], HEAD + tokens.shape[1]), bf16),
        compiler_params=pltpu.CompilerParams(vmem_limit_bytes=12 << 20),
        cost_estimate=pl.CostEstimate(flops=40000000, bytes_accessed=2200000, transcendentals=9000),
        name="cell",
    )(*stored)


def marker_kernel(place, out):
    row = lax.broadcasted_iota(jnp.int32, out.shape, 0)
    out[...] = jnp.where(row == place[0], 1.0, 0.0)


def marker(place, count):
    return pl.pallas_call(
        marker_kernel,
        out_shape=jax.ShapeDtypeStruct((count, HEAD), f32),
        in_specs=[pl.BlockSpec(memory_space=pltpu.SMEM)],
        compiler_params=pltpu.CompilerParams(vmem_limit_bytes=1 << 20),
        cost_estimate=pl.CostEstimate(flops=8000000000, bytes_accessed=16384, transcendentals=0),
        name="marker",
    )(place[None])


def residual_kernel(me, place, second, w0, w1, w2, w3, gain, ids, group, outgoing, own, resid):
    near, tp, seqs, _ = second.shape
    quarter = w0.shape[1]
    heads = jnp.concatenate(
        [
            jnp.concatenate([second[s, k, :, :HEAD] for s in range(near)], axis=0)
            for k in range(tp)
        ],
        axis=1,
    )
    total = jnp.zeros((near * seqs, 1), f32)
    for step, weight in enumerate((w0, w1, w2, w3)):
        k = (me[0] + tp - step) & (tp - 1)
        added = dot(heads, weight[...])
        old = jnp.concatenate([second[s, k, :, HEAD:] for s in range(near)], axis=0)
        values = (old.astype(f32) + added).astype(bf16)
        wide = values.astype(f32)
        total = total + jnp.sum(wide * wide, axis=1, keepdims=True)
        resid[:, pl.ds(pl.multiple_of(k * quarter, quarter), quarter)] = wide
        if step == 0:
            group[:, :quarter] = values
    start = pl.multiple_of(place[0] * seqs, seqs)
    own[...] = group[pl.ds(start, seqs), :quarter]
    scale = lax.rsqrt(total * (1.0 / (tp * quarter)) + epsilon)
    group[...] = (resid[...] * scale * gain[...]).astype(bf16)
    experts = outgoing.shape[0]
    expert = lax.broadcasted_iota(jnp.int32, (experts, seqs), 0)
    chosen = ((expert == ids[0:1, :]) | (expert == ids[1:2, :])).astype(f32).astype(bf16)
    rows = dot(chosen, group[pl.ds(start, seqs), :])
    for k in range(tp):
        outgoing[:, k, :] = rows[:, k * quarter : (k + 1) * quarter].astype(bf16)


def residual(me, place, second, weights, gain, ids, experts):
    near, tp, seqs, _ = second.shape
    quarter = weights[0].shape[1]
    whole = pl.BlockSpec(memory_space=pltpu.VMEM)
    scalar = pl.BlockSpec(memory_space=pltpu.SMEM)
    return pl.pallas_call(
        residual_kernel,
        out_shape=(
            jax.ShapeDtypeStruct((near * seqs, tp * quarter), bf16),
            jax.ShapeDtypeStruct((experts, tp, quarter), bf16),
            jax.ShapeDtypeStruct((seqs, quarter), bf16),
        ),
        in_specs=[scalar, scalar] + [whole] * 7,
        out_specs=(whole, whole, whole),
        scratch_shapes=[pltpu.VMEM((near * seqs, tp * quarter), f32)],
        cost_estimate=pl.CostEstimate(flops=140000000, bytes_accessed=2000000, transcendentals=128),
        compiler_params=pltpu.CompilerParams(vmem_limit_bytes=12 << 20),
        name="residual",
    )(me[None], place[None], second, *weights, gain, ids)


def dense_kernel(group, weights, mix, out):
    far, tp, _, quarter = weights.shape

    def matrix(k, place):
        return weights[:, k, place * SLOT : (place + 1) * SLOT].reshape(far * SLOT, quarter)

    rows = group[...]
    gate, up = 0.0, 0.0
    for k in range(tp):
        part = rows[:, k * quarter : (k + 1) * quarter]
        gate = gate + dot_turned(part, matrix(k, 0))
        up = up + dot_turned(part, matrix(k, 1))
    hidden = (gate * jax.nn.sigmoid(gate) * up).astype(bf16)
    logit = jnp.sum(rows.astype(f32) * mix[...].astype(f32), axis=1, keepdims=True)
    mix_gate = jax.nn.sigmoid(logit)
    for k in range(tp):
        out[:, k * quarter : (k + 1) * quarter] = mix_gate * dot(hidden, matrix(k, 2))


def dense_branch(group, weights, mix):
    return pl.pallas_call(
        dense_kernel,
        out_shape=jax.ShapeDtypeStruct(group.shape, f32),
        compiler_params=pltpu.CompilerParams(vmem_limit_bytes=12 << 20),
        cost_estimate=pl.CostEstimate(flops=100000000, bytes_accessed=1800000, transcendentals=32000),
        name="dense",
    )(group, weights, mix)


def expert_kernel(rows, gate, up, down, out):
    parts, width = rows.shape[1:]
    here = jnp.concatenate([rows[:, k, :] for k in range(parts)], axis=1)
    opened = dot_turned(here, gate[...])
    hidden = opened * jax.nn.sigmoid(opened) * dot_turned(here, up[...])
    result = dot(hidden.astype(bf16), down[...]).astype(bf16)
    for k in range(parts):
        out[:, k, :] = result[:, k * width : (k + 1) * width]


def expert(rows, gate, up, down):
    return pl.pallas_call(
        expert_kernel,
        out_shape=jax.ShapeDtypeStruct(rows.shape, bf16),
        compiler_params=pltpu.CompilerParams(vmem_limit_bytes=12 << 20),
        cost_estimate=pl.CostEstimate(flops=277000000, bytes_accessed=2700000, transcendentals=45000),
        name="expert",
    )(rows, gate, up, down)


def combine_kernel(mine, part, returned, ids, weights, out):
    seqs, quarter = out.shape[1:]
    experts, tp, _ = returned.shape
    expert = lax.broadcasted_iota(jnp.int32, (seqs, experts), 1)
    here = ids[...]
    ahead, behind = upright(weights[0:1]), upright(weights[1:2])
    rows = jnp.concatenate([returned[:, k, :] for k in range(tp)], axis=1)
    first = dot((expert == here[:, 0:1]).astype(f32).astype(bf16), rows)
    second = dot((expert == here[:, 1:2]).astype(f32).astype(bf16), rows)
    moe = ahead * first + behind * second
    for s in range(out.shape[0] // tp):
        for k in range(tp):
            columns = slice(k * quarter, (k + 1) * quarter)
            value = part[s * seqs : (s + 1) * seqs, columns] + mine[s : s + 1, 0:1] * moe[:, columns]
            out[s * tp + k] = value.astype(bf16)


def combine(mine, part, returned, ids, weights, quarter):
    seqs = ids.shape[0]
    whole = pl.BlockSpec(memory_space=pltpu.VMEM)
    count = part.shape[0] // seqs * (part.shape[1] // quarter)
    return pl.pallas_call(
        combine_kernel,
        out_shape=jax.ShapeDtypeStruct((count, seqs, quarter), bf16),
        compiler_params=pltpu.CompilerParams(vmem_limit_bytes=8 << 20),
        name="combine",
    )(mine, part, returned, ids, weights)


def layer(
    tokens,
    gain_mix,
    w_query,
    w_key,
    w_value,
    w_outgate,
    w_input_gate,
    w_forget_gate,
    w_mix_out,
    cell_state,
    norm_state,
    max_state,
    gain_ffn,
    route_ids,
    route_logits,
    expert_gate,
    expert_up,
    expert_down,
    dense_gate,
    dense_up,
    dense_down,
    dense_mix,
):
    seqs, quarter = tokens.shape
    tp = lax.axis_size("x")
    far = lax.axis_size(FAR)
    near = lax.axis_size(NEAR)
    experts = lax.axis_size(EP)
    me = lax.axis_index("x")
    place = lax.axis_index(NEAR)

    sent = pack(tokens, dense_gate.T, dense_up.T, dense_down, dense_mix, tp)
    first = exchange(sent, "x")
    mix_row = first[:, seqs + 3 * SLOT].reshape(1, -1)

    turned_logits = route_logits.T
    route_weight = jax.nn.sigmoid(turned_logits - turned_logits[::-1])
    mine = marker(place, near)

    mix_out = {0: w_mix_out}
    for step in (2, 1, 3):
        mix_out[step] = shifted(w_mix_out, "x", step)

    dense = lax.all_gather(first[:, seqs : seqs + 3 * SLOT].reshape(-1, quarter), FAR)
    dense = dense.reshape(far, tp, 3 * SLOT, quarter)

    sent = cell(
        first,
        gain_mix[None],
        w_query,
        w_key,
        w_value,
        w_outgate,
        w_input_gate.T,
        w_forget_gate.T,
        cell_state[:, 0],
        norm_state[:, 0],
        max_state.T,
        tokens,
        near * tp,
    )
    second = exchange(sent, NEAR + ("x",))
    second = second.reshape(near, tp, seqs, HEAD + quarter)
    group, outgoing, own_resid = residual(
        me, place, second, [mix_out[k] for k in range(tp)], gain_ffn[None], route_ids.T, experts
    )

    received = exchange(outgoing, EP)

    partial = expert(received, expert_gate[0].T, expert_up[0].T, expert_down[0])
    returned = exchange(partial, EP)

    part = dense_branch(group, dense, mix_row)
    part = combine(mine, part, returned, route_ids, route_weight, quarter)
    parts = exchange(part, NEAR + ("x",))
    total = own_resid.astype(f32) + parts.astype(f32).sum(axis=0)
    return total.astype(bf16)


def solution(mesh):
    fine = Mesh(mesh.devices.reshape(4, 2, 4, 2, 2, 4), EP + ("x",))
    return jax.shard_map(
        layer,
        mesh=fine,
        in_specs=(
            P(EP, "x"),
            P(),
            P(None, "x"),
            P(None, "x"),
            P(None, "x"),
            P(None, "x"),
            P(None, "x"),
            P(None, "x"),
            P(None, "x"),
            P(EP, "x", None, None),
            P(EP, "x", None),
            P(EP, "x"),
            P(),
            P(EP, None),
            P(EP, None),
            P(EP, None, "x"),
            P(EP, None, "x"),
            P(EP, "x", None),
            P("x", EP),
            P("x", EP),
            P(EP, "x"),
            P("x"),
        ),
        out_specs=P(EP, "x"),
        check_vma=False,
    )
```

```python
import jax
import jax.numpy as jnp
from jax import lax
from jax.experimental import pallas as pl
from jax.experimental.pallas import tpu as pltpu
from jax.sharding import Mesh, PartitionSpec as P

HEAD = 128

epsilon = 1e-06
f32 = jnp.float32
bf16 = jnp.bfloat16

FAR = ("zh", "yh", "c")
NEAR = ("zl", "yl")
SLOT = 8
EP = ("zh", "zl", "yh", "yl", "c")


def exchange(blocks, axis):
    return lax.all_to_all(blocks, axis, 0, 0, tiled=True)


def dot(a, b):
    return jnp.dot(a, b, preferred_element_type=f32)


def dot_turned(a, b):
    return lax.dot_general(a, b, (((1,), (1,)), ((), ())), preferred_element_type=f32)


def swapped(array, axis, step):
    size = lax.axis_size(axis)
    return lax.ppermute(array, axis, [(i, i ^ step) for i in range(size)])


def upright(row):
    count = row.shape[1]
    square = (count, count)
    same = lax.broadcasted_iota(jnp.int32, square, 0) == lax.broadcasted_iota(jnp.int32, square, 1)
    return jnp.sum(jnp.where(same, jnp.broadcast_to(row, square), 0.0), axis=1, keepdims=True)


def pack_kernel(tokens, gate, up, down, mix, out):
    seqs, quarter = tokens.shape
    count, columns = out.shape[0], gate.shape[0]
    slim = columns // count
    room = out.shape[1] - seqs
    source = jnp.concatenate([gate[...], up[...], down[...]], axis=0)
    row = lax.broadcasted_iota(jnp.int32, (room, 3 * columns), 0)
    column = lax.broadcasted_iota(jnp.int32, (room, 3 * columns), 1)
    slot = row & (SLOT - 1)
    wanted = slot + lax.div(row, SLOT) * columns
    last = lax.broadcasted_iota(jnp.int32, (room, quarter), 0) == 3 * SLOT
    extra = jnp.where(last, jnp.broadcast_to(mix[...].astype(f32)[None], (room, quarter)), 0.0)
    for k in range(count):
        pick = (column == wanted + k * slim) & (slot < slim) & (row < 3 * SLOT)
        out[k, :seqs] = tokens[...]
        out[k, seqs:] = (dot(pick.astype(f32).astype(bf16), source) + extra).astype(bf16)


def pack(tokens, gate, up, down, mix, count):
    seqs, quarter = tokens.shape
    return pl.pallas_call(
        pack_kernel,
        out_shape=jax.ShapeDtypeStruct((count, seqs + 4 * SLOT, quarter), bf16),
        name="pack",
    )(tokens, gate, up, down, mix)


def cell_kernel(first, gain, wq, wk, wv, wo, wi, wf, norm, peak, tokens, state, out):
    seqs = norm.shape[0]
    values = jnp.concatenate([first[k, :seqs] for k in range(first.shape[0])], axis=1).astype(f32)
    scale = lax.rsqrt(jnp.mean(values * values, axis=1, keepdims=True) + epsilon)
    rows = (values * scale * gain[...]).astype(bf16)
    query = dot(rows, wq[...])
    key = dot(rows, wk[...]) * HEAD ** (-0.5)
    value = dot(rows, wv[...])
    gate = jax.nn.sigmoid(dot(rows, wo[...]))
    wide = rows.astype(f32)
    enter = jnp.sum(wide * wi[...].astype(f32), axis=1, keepdims=True)
    forget = jnp.sum(wide * wf[...].astype(f32), axis=1, keepdims=True)
    carried = jnp.minimum(forget, 0.0) - jnp.log1p(jnp.exp(-jnp.abs(forget))) + upright(peak[...])
    stabilizer = jnp.maximum(carried, enter)
    old = jnp.exp(carried - stabilizer)
    new = jnp.exp(enter - stabilizer) * jnp.sum(query * key, axis=1, keepdims=True)
    turned = query.T
    read = [
        jnp.sum(turned[:, b : b + 1] * state[b], axis=0, keepdims=True) for b in range(seqs)
    ]
    numerator = old * jnp.concatenate(read, axis=0) + new * value
    denominator = old * jnp.sum(query * norm[...], axis=1, keepdims=True) + new
    mixed = gate * (numerator / jnp.maximum(jnp.abs(denominator), 1.0))
    mixed = mixed.astype(bf16)
    for k in range(out.shape[0]):
        out[k, :, :HEAD] = mixed
        out[k, :, HEAD:] = tokens[...]


def cell(first, gain, wq, wk, wv, wo, wi, wf, state, norm, peak, tokens, count):
    stored = (first, gain, wq, wk, wv, wo, wi, wf, norm, peak, tokens, state)
    return pl.pallas_call(
        cell_kernel,
        out_shape=jax.ShapeDtypeStruct((count, norm.shape[0], HEAD + tokens.shape[1]), bf16),
        compiler_params=pltpu.CompilerParams(vmem_limit_bytes=12 << 20),
        cost_estimate=pl.CostEstimate(flops=40000000, bytes_accessed=2200000, transcendentals=9000),
        name="cell",
    )(*stored)


def marker_kernel(place, out):
    row = lax.broadcasted_iota(jnp.int32, out.shape, 0)
    out[...] = jnp.where(row == place[0], 1.0, 0.0)


def marker(place, count):
    return pl.pallas_call(
        marker_kernel,
        out_shape=jax.ShapeDtypeStruct((count, HEAD), f32),
        in_specs=[pl.BlockSpec(memory_space=pltpu.SMEM)],
        compiler_params=pltpu.CompilerParams(vmem_limit_bytes=1 << 20),
        cost_estimate=pl.CostEstimate(flops=8000000000, bytes_accessed=16384, transcendentals=0),
        name="marker",
    )(place[None])


def residual_kernel(me, place, second, w0, w1, w2, w3, gain, ids, group, outgoing, own, resid):
    near, tp, seqs, _ = second.shape
    quarter = w0.shape[1]
    heads = jnp.concatenate(
        [
            jnp.concatenate([second[s, k, :, :HEAD] for s in range(near)], axis=0)
            for k in range(tp)
        ],
        axis=1,
    )
    total = jnp.zeros((near * seqs, 1), f32)
    for step, weight in enumerate((w0, w1, w2, w3)):
        k = me[0] ^ step
        added = dot(heads, weight[...])
        old = jnp.concatenate([second[s, k, :, HEAD:] for s in range(near)], axis=0)
        values = (old.astype(f32) + added).astype(bf16)
        wide = values.astype(f32)
        total = total + jnp.sum(wide * wide, axis=1, keepdims=True)
        resid[:, pl.ds(pl.multiple_of(k * quarter, quarter), quarter)] = wide
        if step == 0:
            group[:, :quarter] = values
    start = pl.multiple_of(place[0] * seqs, seqs)
    own[...] = group[pl.ds(start, seqs), :quarter]
    scale = lax.rsqrt(total * (1.0 / (tp * quarter)) + epsilon)
    group[...] = (resid[...] * scale * gain[...]).astype(bf16)
    experts = outgoing.shape[0]
    expert = lax.broadcasted_iota(jnp.int32, (experts, seqs), 0)
    chosen = ((expert == ids[0:1, :]) | (expert == ids[1:2, :])).astype(f32).astype(bf16)
    rows = dot(chosen, group[pl.ds(start, seqs), :])
    for k in range(tp):
        outgoing[:, k, :] = rows[:, k * quarter : (k + 1) * quarter].astype(bf16)


def residual(me, place, second, weights, gain, ids, experts):
    near, tp, seqs, _ = second.shape
    quarter = weights[0].shape[1]
    whole = pl.BlockSpec(memory_space=pltpu.VMEM)
    scalar = pl.BlockSpec(memory_space=pltpu.SMEM)
    return pl.pallas_call(
        residual_kernel,
        out_shape=(
            jax.ShapeDtypeStruct((near * seqs, tp * quarter), bf16),
            jax.ShapeDtypeStruct((experts, tp, quarter), bf16),
            jax.ShapeDtypeStruct((seqs, quarter), bf16),
        ),
        in_specs=[scalar, scalar] + [whole] * 7,
        out_specs=(whole, whole, whole),
        scratch_shapes=[pltpu.VMEM((near * seqs, tp * quarter), f32)],
        cost_estimate=pl.CostEstimate(flops=140000000, bytes_accessed=2000000, transcendentals=128),
        compiler_params=pltpu.CompilerParams(vmem_limit_bytes=12 << 20),
        name="residual",
    )(me[None], place[None], second, *weights, gain, ids)


def dense_kernel(group, weights, mix, out):
    far, tp, _, quarter = weights.shape

    def matrix(k, place):
        return weights[:, k, place * SLOT : (place + 1) * SLOT].reshape(far * SLOT, quarter)

    rows = group[...]
    gate, up = 0.0, 0.0
    for k in range(tp):
        part = rows[:, k * quarter : (k + 1) * quarter]
        gate = gate + dot_turned(part, matrix(k, 0))
        up = up + dot_turned(part, matrix(k, 1))
    hidden = (gate * jax.nn.sigmoid(gate) * up).astype(bf16)
    logit = jnp.sum(rows.astype(f32) * mix[...].astype(f32), axis=1, keepdims=True)
    mix_gate = jax.nn.sigmoid(logit)
    for k in range(tp):
        out[:, k * quarter : (k + 1) * quarter] = mix_gate * dot(hidden, matrix(k, 2))


def dense_branch(group, weights, mix):
    return pl.pallas_call(
        dense_kernel,
        out_shape=jax.ShapeDtypeStruct(group.shape, f32),
        compiler_params=pltpu.CompilerParams(vmem_limit_bytes=12 << 20),
        cost_estimate=pl.CostEstimate(flops=100000000, bytes_accessed=1800000, transcendentals=32000),
        name="dense",
    )(group, weights, mix)


def expert_kernel(rows, gate, up, down, out):
    parts, width = rows.shape[1:]
    here = jnp.concatenate([rows[:, k, :] for k in range(parts)], axis=1)
    opened = dot_turned(here, gate[...])
    hidden = opened * jax.nn.sigmoid(opened) * dot_turned(here, up[...])
    result = dot(hidden.astype(bf16), down[...]).astype(bf16)
    for k in range(parts):
        out[:, k, :] = result[:, k * width : (k + 1) * width]


def expert(rows, gate, up, down):
    return pl.pallas_call(
        expert_kernel,
        out_shape=jax.ShapeDtypeStruct(rows.shape, bf16),
        compiler_params=pltpu.CompilerParams(vmem_limit_bytes=12 << 20),
        cost_estimate=pl.CostEstimate(flops=277000000, bytes_accessed=2700000, transcendentals=45000),
        name="expert",
    )(rows, gate, up, down)


def combine_kernel(mine, part, returned, ids, weights, out):
    seqs, quarter = out.shape[1:]
    experts, tp, _ = returned.shape
    expert = lax.broadcasted_iota(jnp.int32, (seqs, experts), 1)
    here = ids[...]
    ahead, behind = upright(weights[0:1]), upright(weights[1:2])
    rows = jnp.concatenate([returned[:, k, :] for k in range(tp)], axis=1)
    first = dot((expert == here[:, 0:1]).astype(f32).astype(bf16), rows)
    second = dot((expert == here[:, 1:2]).astype(f32).astype(bf16), rows)
    moe = ahead * first + behind * second
    for s in range(out.shape[0] // tp):
        for k in range(tp):
            columns = slice(k * quarter, (k + 1) * quarter)
            value = part[s * seqs : (s + 1) * seqs, columns] + mine[s : s + 1, 0:1] * moe[:, columns]
            out[s * tp + k] = value.astype(bf16)


def combine(mine, part, returned, ids, weights, quarter):
    seqs = ids.shape[0]
    whole = pl.BlockSpec(memory_space=pltpu.VMEM)
    count = part.shape[0] // seqs * (part.shape[1] // quarter)
    return pl.pallas_call(
        combine_kernel,
        out_shape=jax.ShapeDtypeStruct((count, seqs, quarter), bf16),
        compiler_params=pltpu.CompilerParams(vmem_limit_bytes=8 << 20),
        name="combine",
    )(mine, part, returned, ids, weights)


def layer(
    tokens,
    gain_mix,
    w_query,
    w_key,
    w_value,
    w_outgate,
    w_input_gate,
    w_forget_gate,
    w_mix_out,
    cell_state,
    norm_state,
    max_state,
    gain_ffn,
    route_ids,
    route_logits,
    expert_gate,
    expert_up,
    expert_down,
    dense_gate,
    dense_up,
    dense_down,
    dense_mix,
):
    seqs, quarter = tokens.shape
    tp = lax.axis_size("x")
    far = lax.axis_size(FAR)
    near = lax.axis_size(NEAR)
    experts = lax.axis_size(EP)
    me = lax.axis_index("x")
    place = lax.axis_index(NEAR)

    sent = pack(tokens, dense_gate.T, dense_up.T, dense_down, dense_mix, tp)
    first = exchange(sent, "x")
    mix_row = first[:, seqs + 3 * SLOT].reshape(1, -1)

    turned_logits = route_logits.T
    route_weight = jax.nn.sigmoid(turned_logits - turned_logits[::-1])
    mine = marker(place, near)

    mix_out = {0: w_mix_out}
    for step in (2, 1, 3):
        mix_out[step] = swapped(w_mix_out, "x", step)

    dense = lax.all_gather(first[:, seqs : seqs + 3 * SLOT].reshape(-1, quarter), FAR)
    dense = dense.reshape(far, tp, 3 * SLOT, quarter)

    sent = cell(
        first,
        gain_mix[None],
        w_query,
        w_key,
        w_value,
        w_outgate,
        w_input_gate.T,
        w_forget_gate.T,
        cell_state[:, 0],
        norm_state[:, 0],
        max_state.T,
        tokens,
        near * tp,
    )
    second = exchange(sent, NEAR + ("x",))
    second = second.reshape(near, tp, seqs, HEAD + quarter)
    group, outgoing, own_resid = residual(
        me, place, second, [mix_out[k] for k in range(tp)], gain_ffn[None], route_ids.T, experts
    )

    received = exchange(outgoing, EP)

    partial = expert(received, expert_gate[0].T, expert_up[0].T, expert_down[0])
    returned = exchange(partial, EP)

    part = dense_branch(group, dense, mix_row)
    part = combine(mine, part, returned, route_ids, route_weight, quarter)
    parts = exchange(part, NEAR + ("x",))
    total = own_resid.astype(f32) + parts.astype(f32).sum(axis=0)
    return total.astype(bf16)


def solution(mesh):
    fine = Mesh(mesh.devices.reshape(4, 2, 4, 2, 2, 4), EP + ("x",))
    return jax.shard_map(
        layer,
        mesh=fine,
        in_specs=(
            P(EP, "x"),
            P(),
            P(None, "x"),
            P(None, "x"),
            P(None, "x"),
            P(None, "x"),
            P(None, "x"),
            P(None, "x"),
            P(None, "x"),
            P(EP, "x", None, None),
            P(EP, "x", None),
            P(EP, "x"),
            P(),
            P(EP, None),
            P(EP, None),
            P(EP, None, "x"),
            P(EP, None, "x"),
            P(EP, "x", None),
            P("x", EP),
            P("x", EP),
            P(EP, "x"),
            P("x"),
        ),
        out_specs=P(EP, "x"),
        check_vma=False,
    )
```
